32 devices in a mesh: gr: 2 (over x), sp: 8 (over z, y), tp: 2 (over core).
Axes of the slice: x: 2, y: 2, z: 4, core: 2. Of those that a mesh axis runs over, the one named last changes fastest.
Arguments:
- prompt: bfloat16 [2, 2048, 4096], P('gr', 'sp', 'tp'), parts along dimension 0, may hold values from -6 to 6
- key_weight: bfloat16 [4096, 4096], P(None, 'tp'), may hold values from -0.09375 to 0.09375
- value_weight: bfloat16 [4096, 4096], P(None, 'tp'), may hold values from -0.375 to 0.375
- beta_weight: bfloat16 [4096, 32], P(None, 'tp'), may hold values from -0.09375 to 0.09375
- beta_bias: float32 [32], P('tp'), may hold values from -4.5 to -0.5
- decay_rate: float32 [32], P('tp'), may hold values from 0.1 to 3
- new_query: bfloat16 [2, 32, 128], P('gr', 'tp'), parts along dimension 0, may hold values from -6 to 6
- read_gain: float32 [128], replicated, may hold values from 0.1 to 1.9
Outputs:
- state_cache: bfloat16 [2, 32, 128, 128], P('gr', 'tp', 'sp'), parts along dimension 0
- first_read: float32 [2, 32, 128], P('gr', 'tp'), parts along dimension 0
The draws below stay inside these ranges and needn't reach their ends.
There are 2 independent parts, one for each index of `gr`. The reference program is written for one: setup_inputs(seed, part) draws one part's arguments, and reference() takes and returns one part's arrays. A program takes and returns all parts, laid end to end along the dimension named above; an argument that names none is the same for every part. Nothing has to cross between parts.
All inputs are finite; a program needn't handle non-finite values.
Results may differ from the reference program's by a relative error of at most 0.013.
Values may be sent and summed in bfloat16 or wider, within the bound.
A program may use at most 128 MiB of HBM per device.

```python
import math
import jax
import jax.numpy as jnp
from jax import lax

D = 4096
HEADS = 32
HDIM = 128
BLOCK = 64
LEN = 2048


def draw_prompt(key, part):
    shared_key = jax.random.fold_in(key, 11)
    single_key = jax.random.fold_in(key, 12)
    run_count = LEN // BLOCK
    common = 1.5 * jax.random.normal(shared_key, (run_count, 1, D), jnp.float32)
    own_part = 0.75 * jax.random.normal(single_key, (run_count, BLOCK, D), jnp.float32)
    combined = jnp.clip(common + own_part, -6.0, 6.0).reshape(1, LEN, D)
    return combined.astype(jnp.bfloat16)


def level_of(key, extent, split, least, high):
    def one(position, blocks):
        draws = jax.random.uniform(jax.random.fold_in(jax.random.fold_in(key, 6), position), (blocks,), jnp.float32, least / len(split), high / len(split))
        return jnp.repeat(jnp.exp(draws), extent[position] // blocks).reshape((-1,) + (1,) * (len(extent) - position - 1))

    factor_of = one(*split[0])
    for cut in split[1:]:
        factor_of = factor_of * one(*cut)
    return factor_of


def gaussian(own_key, dims, spread, most, split=(), held_as=jnp.bfloat16):
    result = jax.random.normal(own_key, dims, jnp.float32) * spread
    if len(split) > 0:
        result = level_of(own_key, dims, split, -0.22, 0.18) * result
    return jnp.clip(result, min=-most, max=most).astype(held_as)


def setup_inputs(seed: int = 0, part: int = 0) -> dict:
    arg_keys = jax.random.split(jax.random.key(seed), 9)
    own_keys = jax.random.split(jax.random.fold_in(arg_keys[8], part), 9)
    prompt = draw_prompt(jax.random.fold_in(jax.random.fold_in(arg_keys[8], part), 71), part)
    key_weight = gaussian(arg_keys[1], (D, HEADS * HDIM), D ** -0.5, 0.09375, ((1, 2),))
    value_weight = gaussian(arg_keys[2], (D, HEADS * HDIM), (D // 16) ** -0.5, 0.375, ((1, 2),))
    beta_weight = gaussian(arg_keys[3], (D, HEADS), D ** -0.5, 0.09375, ((1, 2),))
    beta_bias = jnp.clip(-4.5 + 4.0 * jax.random.uniform(arg_keys[4], (HEADS,), jnp.float32) ** level_of(arg_keys[4], (HEADS,), ((0, 2),), -0.2, 0.2), -4.5, -0.5)
    decay_rate = jnp.clip(jnp.exp(math.log(3.0) - 3.4011974 * jax.random.uniform(arg_keys[5], (HEADS,), jnp.float32) ** level_of(arg_keys[5], (HEADS,), ((0, 2),), -0.2, 0.2)), 0.1, 3.0)
    new_query = gaussian(own_keys[6], (1, HEADS, HDIM), 1.0, 6.0, ((1, 2),))
    read_gain = jnp.clip(1.0 + 0.18 * jax.random.normal(arg_keys[7], (HDIM,), jnp.float32), 0.1, 1.9)
    return dict(prompt=prompt, key_weight=key_weight, value_weight=value_weight, beta_weight=beta_weight, beta_bias=beta_bias, decay_rate=decay_rate, new_query=new_query, read_gain=read_gain)


def reference(prompt, key_weight, value_weight, beta_weight, beta_bias, decay_rate, new_query, read_gain):
    tokens = prompt[0]
    key_proj = jnp.dot(tokens, key_weight, preferred_element_type=jnp.float32).astype(jnp.bfloat16)
    value_proj = jnp.dot(tokens, value_weight, preferred_element_type=jnp.float32).astype(jnp.bfloat16)
    beta_pre = jnp.dot(tokens, beta_weight, preferred_element_type=jnp.float32)
    key_proj = lax.optimization_barrier(key_proj)
    value_proj = lax.optimization_barrier(value_proj)
    key_rows = key_proj.astype(jnp.float32).reshape(LEN, HEADS, HDIM)
    key_rows = key_rows * lax.rsqrt(lax.optimization_barrier(jnp.sum(key_rows * key_rows, axis=-1, keepdims=True)) + 1.0)
    values = value_proj.astype(jnp.float32).reshape(LEN, HEADS, HDIM)
    strength = jax.nn.sigmoid(beta_pre + beta_bias)
    retain = jnp.exp(-decay_rate / LEN)

    def advance(memory_matrix, inputs):
        single_key_row, value_row, beta_row = inputs
        retrieved_values = jnp.einsum('jg,jgb->jb', single_key_row, memory_matrix, precision=lax.Precision.HIGHEST)
        written_update = beta_row[:, None, None] * single_key_row[:, :, None]
        memory_matrix = retain[:, None, None] * (memory_matrix - written_update * retrieved_values[:, None, :])
        memory_matrix = memory_matrix + written_update * value_row[:, None, :]
        return (memory_matrix, None)
    initial = jnp.zeros((HEADS, HDIM, HDIM), jnp.float32)
    closing_state = lax.scan(advance, initial, (key_rows, values, strength))[0]
    normalized_query = new_query[0].astype(jnp.float32)
    normalized_query = normalized_query * lax.rsqrt(lax.optimization_barrier(jnp.sum(normalized_query * normalized_query, axis=-1, keepdims=True)) + 1.0)
    unscaled_read = jnp.einsum('jg,jgb->jb', normalized_query, closing_state, precision=lax.Precision.HIGHEST)
    read_out = unscaled_read * lax.rsqrt(lax.optimization_barrier(jnp.mean(unscaled_read * unscaled_read, axis=-1, keepdims=True)) + 0.05) * read_gain
    return (closing_state.astype(jnp.bfloat16)[None], read_out[None])
```

```python
import functools

import jax
import jax.numpy as jnp
from jax import lax
from jax.experimental import pallas as pl
from jax.experimental.pallas import tpu as pltpu
from jax.sharding import PartitionSpec as P

MESH = pl.DeviceIdType.MESH
F32 = jnp.float32
BF16 = jnp.bfloat16


def dot(left, right, contract=((1,), (0,))):
    return lax.dot_general(left, right, (contract, ((), ())), preferred_element_type=F32)


def bounds(size):
    levels = (size - 1).bit_length()
    cuts = [0, min(3, levels)]
    while cuts[-1] < levels:
        cuts.append(min(cuts[-1] + 2, levels))
    return tuple(zip(cuts[:-1], cuts[1:]))


def cut_masks(size):
    row = lax.broadcasted_iota(jnp.int32, (size, 2 * size), 0)
    col = lax.rem(lax.broadcasted_iota(jnp.int32, (size, 2 * size), 1), size)
    masks = []
    for low, high in bounds(size):
        together = (row >> high) == (col >> high)
        apart = (row >> low) != (col >> low)
        masks.append((together & apart & (row > col)).astype(F32).astype(BF16))
    return masks, (row == col).astype(F32).astype(BF16)


def spread(x):
    size = x.shape[1] // 2
    zero = jnp.zeros((x.shape[0], size), x.dtype)
    return jnp.concatenate(
        [jnp.concatenate([x[:, :size], zero], axis=1), jnp.concatenate([zero, x[:, size:]], axis=1)], axis=0
    )


def under(x, y):
    return jnp.concatenate([x, y], axis=0)


def mul(x, y):
    return dot(x, spread(y)).astype(BF16)


def span(heads, masks, eye, tick):
    keys_t, rights, grams = [], [], []
    for key, value, strength, fade in heads:
        key = key.astype(F32)
        key = key * lax.rsqrt(jnp.sum(key * key, axis=1, keepdims=True) + 1.0)
        weighted = (key * strength).astype(BF16)
        value = (value.astype(F32) * (strength * fade)).astype(BF16)
        key_t = key.astype(BF16).T
        half = weighted.shape[0] // 2
        keys_t.append(key_t)
        rights.append(jnp.concatenate([value, weighted], axis=1))
        grams.append(mul(jnp.concatenate([weighted[:half], weighted[half:]], axis=1), key_t))
    cuts = masks.shape[0]
    tick()
    ns = [g * masks[0] for g in grams]
    squares = [mul(x, x) for x in ns]
    tick()
    xs = [eye[...] - x for x in ns]
    pairs = [mul(under(q, x), q) for q, x in zip(squares, xs)]
    tick()
    xs = [x + p[half:] for x, p in zip(xs, pairs)]
    xs = [x + mul(x, p[:half]) for x, p in zip(xs, pairs)]
    for cut in range(1, cuts):
        tick()
        last = cut == cuts - 1
        if last:
            both = [mul(under(g * masks[cut], k), x) for g, k, x in zip(grams, keys_t, xs)]
            ns, xs = [b[:half] for b in both], [b[half:] for b in both]
        else:
            ns = [mul(g * masks[cut], x) for g, x in zip(grams, xs)]
        tick()
        pairs = [mul(under(q, x), q) for q, x in zip(ns, xs)]
        tick()
        xs = [x - p[half:] for x, p in zip(xs, pairs)]
        xs = [x + mul(x, p[:half]) for x, p in zip(xs, pairs)]
    if cuts == 1:
        tick()
        xs = [mul(k, x) for k, x in zip(keys_t, xs)]
    tick()
    first = [dot(x[:, :half], r[:half]) for x, r in zip(xs, rights)]
    second = [dot(x[:, half:], r[half:]) for x, r in zip(xs, rights)]
    tick()
    dim = keys_t[0].shape[0]
    out = [a + b - dot(b[:, dim:].astype(BF16), a.astype(BF16)) for a, b in zip(first, second)]
    tick()
    return out


def kernel(
    n, tp, groups, per, dim, together,
    prompt, key_w, value_w, beta_w, bias, decay, query, gain,
    state_out, read_out,
    feat, weights, total, projected, beta_buf, bias_buf, decay_buf, query_buf, gain_buf,
    mask_buf, eye_buf, strength_buf, spans, partner_spans, joined, recv,
    row_stage, row_recv, read_stage, read_recv,
    in_sem, beta_sem, feat_send, feat_recv, weight_sem, pair_send, pair_recv,
    map_send, map_recv, row_send, row_got, read_send, read_got,
):
    me = lax.axis_index("sp")
    core = lax.axis_index("tp")
    seg, part = prompt.shape[1], prompt.shape[2]
    wide = per * dim
    full = seg * n
    stride = n // groups
    half = groups // 2
    parity = lax.rem(me, 2)
    mine = me // stride
    steps = groups // together
    chunk = min(part, 1024)

    away = [half // 2] + [j for j in range(1, half) if j != half // 2] if half > 1 else []
    order = away + [0]
    sequence = [(0, order[0])]
    for j in range(half):
        if j + 1 < half:
            sequence.append((0, order[j + 1]))
        sequence.append((1, order[j]))
    plan = [range(step * together, (step + 1) * together) for step in range(steps)]

    def owner(g):
        return g * stride + (lax.rem(g, 2) if stride > 1 else 0)

    is_owner = me == owner(mine)

    def when_owner(work):
        if stride == 1:
            work()
        else:
            pl.when(is_owner)(work)

    def pair_at(j):
        return lax.rem(mine // 2 + j, half)

    def group_at(index):
        keep, j = sequence[index]
        return 2 * pair_at(j) + (parity if keep else 1 - parity)

    def features_of(d):
        return pl.ds(pl.multiple_of(lax.rem(core + d, tp) * part, part), part)

    def fetch(index, d):
        columns = pl.ds(pl.multiple_of(group_at(index) * wide, wide), wide)
        return [
            pltpu.make_async_copy(
                w.at[features_of(d), columns], weights.at[index, j, d], weight_sem.at[index, j, d]
            )
            for j, w in enumerate((key_w, value_w))
        ]

    def fetch_step(step):
        for d in range(tp):
            for index in plan[step]:
                for copy in fetch(index, d):
                    copy.start()

    own_prompt = pltpu.make_async_copy(prompt.at[0], feat.at[0], in_sem.at[0])
    small = [
        pltpu.make_async_copy(src, dst, in_sem.at[1 + k])
        for k, (src, dst) in enumerate(
            ((bias, bias_buf), (decay, decay_buf), (query, query_buf), (gain, gain_buf))
        )
    ] + [
        pltpu.make_async_copy(beta_w.at[:, features_of(d)], beta_buf.at[d], beta_sem.at[d]) for d in range(tp)
    ]
    own_prompt.start()
    fetch_step(0)
    for copy in small:
        copy.start()
    if steps > 1:
        fetch_step(1)

    barrier = pltpu.get_barrier_semaphore()
    for d in range(1, tp):
        pl.semaphore_signal(barrier, inc=1, device_id={"tp": lax.rem(core + d, tp)}, device_id_type=MESH)
    for d in range(1, n):
        pl.semaphore_signal(barrier, inc=1, device_id={"sp": lax.rem(me + d, n)}, device_id_type=MESH)
    masks, eye = cut_masks(seg // 2)
    for k, mask in enumerate(masks):
        mask_buf[k] = mask
    eye_buf[...] = eye
    own_prompt.wait()
    pl.semaphore_wait(barrier, n - 1 + tp - 1)

    def feature_copy(d):
        return pltpu.make_async_remote_copy(
            src_ref=feat.at[0], dst_ref=feat.at[tp - d],
            send_sem=feat_send.at[d - 1], recv_sem=feat_recv.at[tp - d],
            device_id={"tp": lax.rem(core + d, tp)}, device_id_type=MESH,
        )

    for d in range(1, tp):
        feature_copy(d).start()

    for index in plan[0]:
        for j, copy in enumerate(fetch(index, 0)):
            copy.wait()
            total[index, j] = dot(feat[0], weights[index, j, 0])
    for copy in small:
        copy.wait()
    before = dot(feat[0], beta_buf[0], ((1,), (1,)))
    for d in range(1, tp):
        feature_copy(tp - d).wait_recv()
        before += dot(feat[d], beta_buf[d], ((1,), (1,)))
    strength_buf[...] = jax.nn.sigmoid(before + bias_buf[...])
    for index in plan[0]:
        for d in range(1, tp):
            for copy in fetch(index, d):
                copy.wait()
    for index in plan[0]:
        for j in range(2):
            acc = total[index, j]
            for d in range(1, tp):
                acc += dot(feat[d], weights[index, j, d])
            projected[index, j] = acc.astype(BF16)

    def pair_copy(index, j):
        return pltpu.make_async_remote_copy(
            src_ref=spans.at[index], dst_ref=partner_spans.at[j],
            send_sem=pair_send.at[j], recv_sem=pair_recv.at[j],
            device_id={"sp": me + 1 - 2 * parity}, device_id_type=MESH,
        )

    def map_copy(j, slot):
        return pltpu.make_async_remote_copy(
            src_ref=joined.at[j], dst_ref=recv.at[slot],
            send_sem=map_send.at[j], recv_sem=map_recv.at[slot],
            device_id={"sp": owner(2 * pair_at(j) + parity)}, device_id_type=MESH,
        )

    def is_away(j):
        return owner(2 * pair_at(j) + parity) != me

    def pass_on(step):
        for index in plan[step]:
            keep, j = sequence[index]
            if not keep:
                pair_copy(index, j).start()
        for index in plan[step]:
            keep, j = sequence[index]
            if keep:
                pair_copy(index, j).wait_recv()
                for h in range(per):
                    ours, theirs = spans[index, h], partner_spans[j, h]
                    early = jnp.where(parity == 1, theirs, ours)
                    late = jnp.where(parity == 1, ours, theirs)
                    both = early.astype(F32) + late.astype(F32) - dot(late[:, dim:], early)
                    joined[j, h] = both.astype(BF16)
                if j or stride > 1:
                    @pl.when(is_away(j))
                    def _():
                        map_copy(j, me // 2).start()

    def projection(step):
        for index in plan[step]:
            for j in range(2):
                acc = None
                for d in range(tp):
                    for low in range(0, part, chunk):
                        piece = dot(
                            feat[d, :, low:low + chunk], weights[index, j, d, low:low + chunk, :]
                        )
                        acc = piece if acc is None else acc + piece
                        if d == tp - 1 and low + chunk == part:
                            projected[index, j] = acc.astype(BF16)
                        yield

    ticks = 2 + 3 * len(masks) + 1
    units = together * 2 * tp * (part // chunk)
    for step in range(steps):
        if step > 0:
            pass_on(step - 1)
        if step + 2 < steps:
            fetch_step(step + 2)
        filler = iter(())
        if step + 1 < steps:
            for index in plan[step + 1]:
                for d in range(tp):
                    for copy in fetch(index, d):
                        copy.wait()
            filler = projection(step + 1)
        done = [0, 0]

        def tick():
            done[0] += 1
            while done[1] * ticks < done[0] * units:
                done[1] += 1
                next(filler, None)

        strengths = strength_buf[...]
        rates = decay_buf[...]
        lane = lax.broadcasted_iota(jnp.int32, strengths.shape, 1)
        rest = full - 1 - me * seg - lax.broadcasted_iota(jnp.int32, (seg, 1), 0)
        rest = rest.astype(F32) * (1.0 / full)
        heads = []
        for index in plan[step]:
            keys, values = projected[index, 0], projected[index, 1]
            for h in range(per):
                head = group_at(index) * per + h
                strength = jnp.sum(jnp.where(lane == head, strengths, 0.0), axis=1, keepdims=True)
                rate = jnp.sum(jnp.where(lane[:1] == head, rates, 0.0), axis=1, keepdims=True)
                fade = jnp.exp(-rate * rest)
                cols = slice(h * dim, (h + 1) * dim)
                heads.append((keys[:, cols], values[:, cols], strength, fade))
        results = span(heads, mask_buf, eye_buf, tick)
        for _ in filler:
            pass
        for k, result in enumerate(results):
            spans[plan[step][k // per], k % per] = result.astype(BF16)
    pass_on(steps - 1)
    recv[me // 2] = joined[0]

    rows = dim // n

    def row_copy(q, slot):
        return pltpu.make_async_remote_copy(
            src_ref=row_stage.at[q], dst_ref=row_recv.at[slot],
            send_sem=row_send.at[q], recv_sem=row_got.at[slot],
            device_id={"sp": q}, device_id_type=MESH,
        )

    def read_copy(q, slot):
        return pltpu.make_async_remote_copy(
            src_ref=read_stage, dst_ref=read_recv.at[slot],
            send_sem=read_send.at[q], recv_sem=read_got.at[slot],
            device_id={"sp": q}, device_id_type=MESH,
        )

    def finish():
        def link(p, states):
            @pl.when(p != me // 2)
            def _():
                map_copy(0, p).wait_recv()

            new = []
            for h in range(per):
                write, drop = recv[p, h, :, :dim].astype(F32), recv[p, h, :, dim:]
                high = states[h].astype(BF16)
                low = (states[h] - high.astype(F32)).astype(BF16)
                new.append(states[h] + (write - dot(drop, high) - dot(drop, low)))
            return tuple(new)

        states = lax.fori_loop(0, n // 2, link, tuple(jnp.zeros((dim, dim), F32) for _ in range(per)))
        for h in range(per):
            cast = states[h].astype(BF16)
            for q in range(n):
                row_stage[q, h] = cast[q * rows:(q + 1) * rows]
        unit = query_buf[0].astype(F32)
        unit = unit * lax.rsqrt(jnp.sum(unit * unit, axis=1, keepdims=True) + 1.0)
        which = lax.broadcasted_iota(jnp.int32, unit.shape, 0)
        for h in range(per):
            row = jnp.sum(jnp.where(which == mine * per + h, unit, 0.0), axis=0, keepdims=True)
            raw = jnp.dot(
                jnp.broadcast_to(row, (8, dim)), states[h],
                precision=lax.Precision.HIGHEST, preferred_element_type=F32,
            )[0:1]
            raw = raw * lax.rsqrt(jnp.mean(raw * raw, axis=1, keepdims=True) + 0.05) * gain_buf[...]
            read_stage[h:h + 1] = raw
        for d in range(1, n):
            row_copy(lax.rem(me + d, n), mine).start()
        for d in range(1, n):
            read_copy(lax.rem(me + d, n), mine).start()
        row_recv[mine] = row_stage[me]
        read_recv[mine] = read_stage[...]

    when_owner(finish)

    for g in range(groups):
        @pl.when(me != owner(g))
        def _():
            row_copy(me, g).wait_recv()
            read_copy(me, g).wait_recv()

        for h in range(per):
            state_out[0, g * per + h] = row_recv[g, h]
        read_out[0, g * per:(g + 1) * per] = read_recv[g]

    for d in range(1, tp):
        feature_copy(d).wait_send()
    for j in range(half):
        pair_copy(0, j).wait_send()
        if j or stride > 1:
            @pl.when(is_away(j))
            def _():
                map_copy(j, 0).wait_send()

    def sent():
        for d in range(1, n):
            row_copy(lax.rem(me + d, n), mine).wait_send()
            read_copy(lax.rem(me + d, n), mine).wait_send()

    when_owner(sent)


def solution(mesh):
    n, tp = mesh.shape["sp"], mesh.shape["tp"]

    def shards(prompt, key_w, value_w, beta_w, bias, decay, query, gain):
        seg, part = prompt.shape[1:]
        depth = key_w.shape[0]
        heads = beta_w.shape[1]
        dim = key_w.shape[1] // heads
        per = max(1, heads // n)
        groups = heads // per
        wide = per * dim
        rows = dim // n
        block = seg // 2
        cuts = len(bounds(block))
        dma = pltpu.SemaphoreType.DMA
        vmem = pl.BlockSpec(memory_space=pltpu.VMEM)
        hbm = pl.BlockSpec(memory_space=pl.ANY)
        half = groups // 2
        together = min(2, groups)
        return pl.pallas_call(
            functools.partial(kernel, n, tp, groups, per, dim, together),
            out_shape=(
                jax.ShapeDtypeStruct((1, heads, rows, dim), BF16),
                jax.ShapeDtypeStruct((1, heads, dim), F32),
            ),
            in_specs=[hbm] * 8,
            out_specs=(vmem, vmem),
            scratch_shapes=[
                pltpu.VMEM((tp, seg, part), BF16),
                pltpu.VMEM((groups, 2, tp, part, wide), BF16),
                pltpu.VMEM((together, 2, seg, wide), F32),
                pltpu.VMEM((groups, 2, seg, wide), BF16),
                pltpu.VMEM((tp, heads, part), BF16),
                pltpu.VMEM((1, heads), F32),
                pltpu.VMEM((1, heads), F32),
                pltpu.VMEM((1, heads, dim), BF16),
                pltpu.VMEM((1, dim), F32),
                pltpu.VMEM((cuts, block, seg), BF16),
                pltpu.VMEM((block, seg), BF16),
                pltpu.VMEM((seg, heads), F32),
                pltpu.VMEM((groups, per, dim, 2 * dim), BF16),
                pltpu.VMEM((half, per, dim, 2 * dim), BF16),
                pltpu.VMEM((half, per, dim, 2 * dim), BF16),
                pltpu.VMEM((n // 2, per, dim, 2 * dim), BF16),
                pltpu.VMEM((n, per, rows, dim), BF16),
                pltpu.VMEM((groups, per, rows, dim), BF16),
                pltpu.VMEM((per, dim), F32),
                pltpu.VMEM((groups, per, dim), F32),
                dma((5,)),
                dma((tp,)),
                dma((tp - 1,)),
                dma((tp,)),
                dma((groups, 2, tp)),
                dma((half,)),
                dma((half,)),
                dma((half,)),
                dma((n // 2,)),
                dma((n,)),
                dma((groups,)),
                dma((n,)),
                dma((groups,)),
            ],
            compiler_params=pltpu.CompilerParams(
                collective_id=0, has_side_effects=True, vmem_limit_bytes=60 * 2**20
            ),
        )(
            prompt, key_w, value_w, beta_w.T, bias.reshape(1, heads), decay.reshape(1, heads),
            query, gain.reshape(1, dim),
        )

    return jax.shard_map(
        shards,
        mesh=mesh,
        in_specs=(
            P("gr", "sp", "tp"),
            P(None, "tp"),
            P(None, "tp"),
            P(None, "tp"),
            P("tp"),
            P("tp"),
            P("gr", "tp", None),
            P(),
        ),
        out_specs=(P("gr", "tp", "sp", None), P("gr", "tp", None)),
        check_vma=False,
    )
```

```python
import functools

import jax
import jax.numpy as jnp
from jax import lax
from jax.experimental import pallas as pl
from jax.experimental.pallas import tpu as pltpu
from jax.sharding import PartitionSpec as P

MESH = pl.DeviceIdType.MESH
F32 = jnp.float32
BF16 = jnp.bfloat16


def dot(left, right, contract=((1,), (0,))):
    return lax.dot_general(left, right, (contract, ((), ())), preferred_element_type=F32)


def bounds(size):
    levels = (size - 1).bit_length()
    cuts = [0, min(3, levels)]
    while cuts[-1] < levels:
        cuts.append(min(cuts[-1] + 2, levels))
    return tuple(zip(cuts[:-1], cuts[1:]))


def cut_masks(size):
    row = lax.broadcasted_iota(jnp.int32, (size, 2 * size), 0)
    col = lax.rem(lax.broadcasted_iota(jnp.int32, (size, 2 * size), 1), size)
    masks = []
    for low, high in bounds(size):
        together = (row >> high) == (col >> high)
        apart = (row >> low) != (col >> low)
        masks.append((together & apart & (row > col)).astype(F32).astype(BF16))
    return masks, (row == col).astype(F32).astype(BF16)


def spread(x):
    size = x.shape[1] // 2
    zero = jnp.zeros((x.shape[0], size), x.dtype)
    return jnp.concatenate(
        [jnp.concatenate([x[:, :size], zero], axis=1), jnp.concatenate([zero, x[:, size:]], axis=1)], axis=0
    )


def under(x, y):
    return jnp.concatenate([x, y], axis=0)


def mul(x, y):
    return dot(x, spread(y)).astype(BF16)


def span(heads, masks, eye, tick):
    keys_t, rights, grams = [], [], []
    for key, value, strength, fade in heads:
        key = key.astype(F32)
        key = key * lax.rsqrt(jnp.sum(key * key, axis=1, keepdims=True) + 1.0)
        weighted = (key * strength).astype(BF16)
        value = (value.astype(F32) * (strength * fade)).astype(BF16)
        key_t = key.astype(BF16).T
        half = weighted.shape[0] // 2
        keys_t.append(key_t)
        rights.append(jnp.concatenate([value, weighted], axis=1))
        grams.append(mul(jnp.concatenate([weighted[:half], weighted[half:]], axis=1), key_t))
    cuts = masks.shape[0]
    tick()
    ns = [g * masks[0] for g in grams]
    squares = [mul(x, x) for x in ns]
    tick()
    xs = [eye[...] - x for x in ns]
    pairs = [mul(under(q, x), q) for q, x in zip(squares, xs)]
    tick()
    xs = [x + p[half:] for x, p in zip(xs, pairs)]
    xs = [x + mul(x, p[:half]) for x, p in zip(xs, pairs)]
    for cut in range(1, cuts):
        tick()
        last = cut == cuts - 1
        if last:
            both = [mul(under(g * masks[cut], k), x) for g, k, x in zip(grams, keys_t, xs)]
            ns, xs = [b[:half] for b in both], [b[half:] for b in both]
        else:
            ns = [mul(g * masks[cut], x) for g, x in zip(grams, xs)]
        tick()
        pairs = [mul(under(q, x), q) for q, x in zip(ns, xs)]
        tick()
        xs = [x - p[half:] for x, p in zip(xs, pairs)]
        xs = [x + mul(x, p[:half]) for x, p in zip(xs, pairs)]
    if cuts == 1:
        tick()
        xs = [mul(k, x) for k, x in zip(keys_t, xs)]
    tick()
    first = [dot(x[:, :half], r[:half]) for x, r in zip(xs, rights)]
    second = [dot(x[:, half:], r[half:]) for x, r in zip(xs, rights)]
    tick()
    dim = keys_t[0].shape[0]
    out = [a + b - dot(b[:, dim:].astype(BF16), a.astype(BF16)) for a, b in zip(first, second)]
    tick()
    return out


def kernel(
    n, tp, groups, per, dim,
    prompt, key_w, value_w, beta_w, bias, decay, query, gain,
    state_out, read_out,
    feat, weights, total, projected, beta_buf, bias_buf, decay_buf, query_buf, gain_buf,
    mask_buf, eye_buf, strength_buf, spans, partner_spans, joined, recv,
    row_stage, row_recv, read_stage, read_recv,
    in_sem, beta_sem, feat_send, feat_recv, weight_sem, pair_send, pair_recv,
    map_send, map_recv, row_send, row_got, read_send, read_got,
):
    me = lax.axis_index("sp")
    core = lax.axis_index("tp")
    seg, part = prompt.shape[1], prompt.shape[2]
    wide = per * dim
    full = seg * n
    stride = n // groups
    half = groups // 2
    parity = lax.rem(me, 2)
    mine = me // stride
    chunk = min(part, 1024)

    order = list(range(half // 2, half)) + list(range(half // 2 - 1, -1, -1))
    sequence = [(0, order[0])]
    for j in range(half):
        if j + 1 < half:
            sequence.append((0, order[j + 1]))
        sequence.append((1, order[j]))
    plan = [range(1)] + [range(k, k + 2) for k in range(1, groups - 1, 2)] + [range(groups - 1, groups)]
    steps = len(plan)
    early = 1 + len(plan[1])

    def owner(g):
        return g * stride + (lax.rem(g, 2) if stride > 1 else 0)

    is_owner = me == owner(mine)

    def when_owner(work):
        if stride == 1:
            work()
        else:
            pl.when(is_owner)(work)

    def pair_at(j):
        pair = mine // 2
        if half & (half - 1):
            return lax.rem(pair + j, half)
        place = pair
        for bit in range(half.bit_length()):
            if j >> bit & 1:
                place += (1 - 2 * lax.rem(pair // 2**bit, 2)) * 2**bit
        return place

    def group_at(index):
        keep, j = sequence[index]
        return 2 * pair_at(j) + (parity if keep else 1 - parity)

    def features_of(d):
        return pl.ds(pl.multiple_of(lax.rem(core + d, tp) * part, part), part)

    def fetch(index, d):
        columns = pl.ds(pl.multiple_of(group_at(index) * wide, wide), wide)
        return [
            pltpu.make_async_copy(
                w.at[features_of(d), columns], weights.at[index, j, d], weight_sem.at[index, j, d]
            )
            for j, w in enumerate((key_w, value_w))
        ]

    def fetch_step(step, ds=None):
        for d in ds or range(tp):
            for index in plan[step]:
                for copy in fetch(index, d):
                    copy.start()

    own_prompt = pltpu.make_async_copy(prompt.at[0], feat.at[0], in_sem.at[0])
    small = [
        pltpu.make_async_copy(src, dst, in_sem.at[1 + k])
        for k, (src, dst) in enumerate(
            ((bias, bias_buf), (decay, decay_buf), (query, query_buf), (gain, gain_buf))
        )
    ] + [
        pltpu.make_async_copy(beta_w.at[:, features_of(d)], beta_buf.at[d], beta_sem.at[d]) for d in range(tp)
    ]
    own_prompt.start()
    fetch_step(0, range(1))
    for copy in small:
        copy.start()
    fetch_step(1, range(1))

    barrier = pltpu.get_barrier_semaphore()
    for d in range(1, tp):
        pl.semaphore_signal(barrier, inc=1, device_id={"tp": lax.rem(core + d, tp)}, device_id_type=MESH)
    for d in range(1, n):
        pl.semaphore_signal(barrier, inc=1, device_id={"sp": lax.rem(me + d, n)}, device_id_type=MESH)
    masks, eye = cut_masks(seg // 2)
    for k, mask in enumerate(masks):
        mask_buf[k] = mask
    eye_buf[...] = eye
    own_prompt.wait()
    pl.semaphore_wait(barrier, n - 1 + tp - 1)

    def feature_copy(d):
        return pltpu.make_async_remote_copy(
            src_ref=feat.at[0], dst_ref=feat.at[tp - d],
            send_sem=feat_send.at[d - 1], recv_sem=feat_recv.at[tp - d],
            device_id={"tp": lax.rem(core + d, tp)}, device_id_type=MESH,
        )

    for d in range(1, tp):
        feature_copy(d).start()
    fetch_step(0, range(1, tp))
    fetch_step(1, range(1, tp))

    def begin(step):
        for index in plan[step]:
            for copy in fetch(index, 0):
                copy.wait()
        for index in plan[step]:
            for j in range(2):
                total[index, j] = dot(feat[0], weights[index, j, 0])

    begin(0)
    if steps > 2:
        fetch_step(2)
    for copy in small:
        copy.wait()
    begin(1)
    before = dot(feat[0], beta_buf[0], ((1,), (1,)))
    for index in plan[0]:
        for d in range(1, tp):
            for copy in fetch(index, d):
                copy.wait()
    for d in range(1, tp):
        feature_copy(tp - d).wait_recv()
    for d in range(1, tp):
        before += dot(feat[d], beta_buf[d], ((1,), (1,)))
    strength_buf[...] = jax.nn.sigmoid(before + bias_buf[...])
    for index in plan[0]:
        for j in range(2):
            acc = total[index, j]
            for d in range(1, tp):
                acc += dot(feat[d], weights[index, j, d])
            projected[index, j] = acc.astype(BF16)

    def pair_copy(index, j):
        return pltpu.make_async_remote_copy(
            src_ref=spans.at[index], dst_ref=partner_spans.at[j],
            send_sem=pair_send.at[j], recv_sem=pair_recv.at[j],
            device_id={"sp": me + 1 - 2 * parity}, device_id_type=MESH,
        )

    def map_copy(j, slot):
        return pltpu.make_async_remote_copy(
            src_ref=joined.at[j], dst_ref=recv.at[slot],
            send_sem=map_send.at[j], recv_sem=map_recv.at[slot],
            device_id={"sp": owner(2 * pair_at(j) + parity)}, device_id_type=MESH,
        )

    def is_away(j):
        return owner(2 * pair_at(j) + parity) != me

    def pass_on(step):
        for index in plan[step]:
            keep, j = sequence[index]
            if not keep:
                pair_copy(index, j).start()
        for index in plan[step]:
            keep, j = sequence[index]
            if keep:
                pair_copy(index, j).wait_recv()
                for h in range(per):
                    ours, theirs = spans[index, h], partner_spans[j, h]
                    early = jnp.where(parity == 1, theirs, ours)
                    late = jnp.where(parity == 1, ours, theirs)
                    both = early.astype(F32) + late.astype(F32) - dot(late[:, dim:], early)
                    joined[j, h] = both.astype(BF16)
                if j or stride > 1:
                    @pl.when(is_away(j))
                    def _():
                        map_copy(j, me // 2).start()

    def projection(step):
        for index in plan[step]:
            for j in range(2):
                acc = total[index, j] if index < early else None
                for d in range(1 if index < early else 0, tp):
                    for low in range(0, part, chunk):
                        piece = dot(
                            feat[d, :, low:low + chunk], weights[index, j, d, low:low + chunk, :]
                        )
                        acc = piece if acc is None else acc + piece
                        if d == tp - 1 and low + chunk == part:
                            projected[index, j] = acc.astype(BF16)
                        yield

    ticks = 2 + 3 * len(masks) + 1
    for step in range(steps):
        if step > 0:
            pass_on(step - 1)
        if 2 < step + 2 < steps:
            fetch_step(step + 2)
        filler, units = iter(()), 0
        if step + 1 < steps:
            skip = 1 if step == 0 else 0
            units = len(plan[step + 1]) * 2 * (tp - skip) * (part // chunk)
            for index in plan[step + 1]:
                for d in range(skip, tp):
                    for copy in fetch(index, d):
                        copy.wait()
            filler = projection(step + 1)
        done = [0, 0]

        def tick():
            done[0] += 1
            while done[1] * ticks < done[0] * units:
                done[1] += 1
                next(filler, None)

        strengths = strength_buf[...]
        rates = decay_buf[...]
        lane = lax.broadcasted_iota(jnp.int32, strengths.shape, 1)
        rest = full - 1 - me * seg - lax.broadcasted_iota(jnp.int32, (seg, 1), 0)
        rest = rest.astype(F32) * (1.0 / full)
        heads = []
        for index in plan[step]:
            keys, values = projected[index, 0], projected[index, 1]
            for h in range(per):
                head = group_at(index) * per + h
                strength = jnp.sum(jnp.where(lane == head, strengths, 0.0), axis=1, keepdims=True)
                rate = jnp.sum(jnp.where(lane[:1] == head, rates, 0.0), axis=1, keepdims=True)
                fade = jnp.exp(-rate * rest)
                cols = slice(h * dim, (h + 1) * dim)
                heads.append((keys[:, cols], values[:, cols], strength, fade))
        results = span(heads, mask_buf, eye_buf, tick)
        for _ in filler:
            pass
        for k, result in enumerate(results):
            spans[plan[step][0] + k // per, k % per] = result.astype(BF16)
    pass_on(steps - 1)
    recv[me // 2] = joined[0]

    rows = dim // n

    def row_copy(q, slot):
        return pltpu.make_async_remote_copy(
            src_ref=row_stage.at[q], dst_ref=row_recv.at[slot],
            send_sem=row_send.at[q], recv_sem=row_got.at[slot],
            device_id={"sp": q}, device_id_type=MESH,
        )

    def read_copy(q, slot):
        return pltpu.make_async_remote_copy(
            src_ref=read_stage, dst_ref=read_recv.at[slot],
            send_sem=read_send.at[q], recv_sem=read_got.at[slot],
            device_id={"sp": q}, device_id_type=MESH,
        )

    def finish():
        unit = query_buf[0].astype(F32)
        unit = unit * lax.rsqrt(jnp.sum(unit * unit, axis=1, keepdims=True) + 1.0)
        which = lax.broadcasted_iota(jnp.int32, unit.shape, 0)
        asks = []
        for h in range(per):
            row = jnp.sum(jnp.where(which == mine * per + h, unit, 0.0), axis=0, keepdims=True)
            asks.append(jnp.broadcast_to(row, (dim, dim)).T)

        def arrive(p):
            @pl.when(p != me // 2)
            def _():
                map_copy(0, p).wait_recv()

        arrive(0)
        states = [recv[0, h, :, :dim].astype(F32) for h in range(per)]
        for p in range(1, n // 2):
            arrive(p)
            for h in range(per):
                write, drop = recv[p, h, :, :dim].astype(F32), recv[p, h, :, dim:]
                high = states[h].astype(BF16)
                low = (states[h] - high.astype(F32)).astype(BF16)
                states[h] = states[h] + (write - dot(drop, high) - dot(drop, low))
        for h in range(per):
            cast = states[h].astype(BF16)
            for q in range(n):
                row_stage[q, h] = cast[q * rows:(q + 1) * rows]
        for d in range(n - 1, 0, -1):
            row_copy(lax.rem(me + d, n), mine).start()
        for h in range(per):
            raw = jnp.sum(asks[h] * states[h], axis=0, keepdims=True)
            raw = raw * lax.rsqrt(jnp.mean(raw * raw, axis=1, keepdims=True) + 0.05) * gain_buf[...]
            read_stage[h:h + 1] = raw
        for d in range(1, n):
            read_copy(lax.rem(me + d, n), mine).start()
        row_recv[mine] = row_stage[me]
        read_recv[mine] = read_stage[...]

    when_owner(finish)

    for g in range(groups):
        @pl.when(me != owner(g))
        def _():
            row_copy(me, g).wait_recv()
            read_copy(me, g).wait_recv()

        for h in range(per):
            state_out[0, g * per + h] = row_recv[g, h]
        read_out[0, g * per:(g + 1) * per] = read_recv[g]

    for d in range(1, tp):
        feature_copy(d).wait_send()
    for j in range(half):
        pair_copy(0, j).wait_send()
        if j or stride > 1:
            @pl.when(is_away(j))
            def _():
                map_copy(j, 0).wait_send()

    def sent():
        for d in range(1, n):
            row_copy(lax.rem(me + d, n), mine).wait_send()
            read_copy(lax.rem(me + d, n), mine).wait_send()

    when_owner(sent)


def solution(mesh):
    n, tp = mesh.shape["sp"], mesh.shape["tp"]

    def shards(prompt, key_w, value_w, beta_w, bias, decay, query, gain):
        seg, part = prompt.shape[1:]
        depth = key_w.shape[0]
        heads = beta_w.shape[1]
        dim = key_w.shape[1] // heads
        per = max(1, heads // n)
        groups = heads // per
        wide = per * dim
        rows = dim // n
        block = seg // 2
        cuts = len(bounds(block))
        dma = pltpu.SemaphoreType.DMA
        vmem = pl.BlockSpec(memory_space=pltpu.VMEM)
        hbm = pl.BlockSpec(memory_space=pl.ANY)
        half = groups // 2
        return pl.pallas_call(
            functools.partial(kernel, n, tp, groups, per, dim),
            out_shape=(
                pltpu.VMEM((1, heads, rows, dim), BF16),
                pltpu.VMEM((1, heads, dim), F32),
            ),
            in_specs=[hbm] * 8,
            out_specs=(vmem, vmem),
            scratch_shapes=[
                pltpu.VMEM((tp, seg, part), BF16),
                pltpu.VMEM((groups, 2, tp, part, wide), BF16),
                pltpu.VMEM((3, 2, seg, wide), F32),
                pltpu.VMEM((groups, 2, seg, wide), BF16),
                pltpu.VMEM((tp, heads, part), BF16),
                pltpu.VMEM((1, heads), F32),
                pltpu.VMEM((1, heads), F32),
                pltpu.VMEM((1, heads, dim), BF16),
                pltpu.VMEM((1, dim), F32),
                pltpu.VMEM((cuts, block, seg), BF16),
                pltpu.VMEM((block, seg), BF16),
                pltpu.VMEM((seg, heads), F32),
                pltpu.VMEM((groups, per, dim, 2 * dim), BF16),
                pltpu.VMEM((half, per, dim, 2 * dim), BF16),
                pltpu.VMEM((half, per, dim, 2 * dim), BF16),
                pltpu.VMEM((n // 2, per, dim, 2 * dim), BF16),
                pltpu.VMEM((n, per, rows, dim), BF16),
                pltpu.VMEM((groups, per, rows, dim), BF16),
                pltpu.VMEM((per, dim), F32),
                pltpu.VMEM((groups, per, dim), F32),
                dma((5,)),
                dma((tp,)),
                dma((tp - 1,)),
                dma((tp,)),
                dma((groups, 2, tp)),
                dma((half,)),
                dma((half,)),
                dma((half,)),
                dma((n // 2,)),
                dma((n,)),
                dma((groups,)),
                dma((n,)),
                dma((groups,)),
            ],
            compiler_params=pltpu.CompilerParams(
                collective_id=0, has_side_effects=True, vmem_limit_bytes=60 * 2**20
            ),
        )(
            prompt, key_w, value_w, beta_w.T, bias.reshape(1, heads), decay.reshape(1, heads),
            query, gain.reshape(1, dim),
        )

    return jax.shard_map(
        shards,
        mesh=mesh,
        in_specs=(
            P("gr", "sp", "tp"),
            P(None, "tp"),
            P(None, "tp"),
            P(None, "tp"),
            P("tp"),
            P("tp"),
            P("gr", "tp", None),
            P(),
        ),
        out_specs=(P("gr", "tp", "sp", None), P("gr", "tp", None)),
        check_vma=False,
    )
```

```python
import functools

import jax
import jax.numpy as jnp
from jax import lax
from jax.experimental import pallas as pl
from jax.experimental.pallas import tpu as pltpu
from jax.sharding import PartitionSpec as P

MESH = pl.DeviceIdType.MESH
F32 = jnp.float32
BF16 = jnp.bfloat16


def dot(left, right, contract=((1,), (0,))):
    return lax.dot_general(left, right, (contract, ((), ())), preferred_element_type=F32)


def bounds(size):
    levels = (size - 1).bit_length()
    cuts = [0, min(3, levels)]
    while cuts[-1] < levels:
        cuts.append(min(cuts[-1] + 2, levels))
    return tuple(zip(cuts[:-1], cuts[1:]))


def cut_masks(size):
    row = lax.broadcasted_iota(jnp.int32, (size, 2 * size), 0)
    col = lax.rem(lax.broadcasted_iota(jnp.int32, (size, 2 * size), 1), size)
    masks = []
    for low, high in bounds(size):
        together = (row >> high) == (col >> high)
        apart = (row >> low) != (col >> low)
        masks.append((together & apart & (row > col)).astype(F32).astype(BF16))
    return masks, (row == col).astype(F32).astype(BF16)


def spread(x):
    size = x.shape[1] // 2
    zero = jnp.zeros((x.shape[0], size), x.dtype)
    return jnp.concatenate(
        [jnp.concatenate([x[:, :size], zero], axis=1), jnp.concatenate([zero, x[:, size:]], axis=1)], axis=0
    )


def under(x, y):
    return jnp.concatenate([x, y], axis=0)


def mul(x, y):
    return dot(x, spread(y)).astype(BF16)


def span(heads, masks, eye, tick):
    keys_t, rights, grams = [], [], []
    for key, value, strength, fade in heads:
        key = key.astype(F32)
        key = key * lax.rsqrt(jnp.sum(key * key, axis=1, keepdims=True) + 1.0)
        weighted = (key * strength).astype(BF16)
        value = (value.astype(F32) * (strength * fade)).astype(BF16)
        key_t = key.astype(BF16).T
        half = weighted.shape[0] // 2
        keys_t.append(key_t)
        rights.append(jnp.concatenate([value, weighted], axis=1))
        grams.append(mul(jnp.concatenate([weighted[:half], weighted[half:]], axis=1), key_t))
    cuts = masks.shape[0]
    tick()
    ns = [g * masks[0] for g in grams]
    squares = [mul(x, x) for x in ns]
    tick()
    xs = [eye[...] - x for x in ns]
    pairs = [mul(under(q, x), q) for q, x in zip(squares, xs)]
    tick()
    xs = [x + p[half:] for x, p in zip(xs, pairs)]
    xs = [x + mul(x, p[:half]) for x, p in zip(xs, pairs)]
    for cut in range(1, cuts):
        tick()
        last = cut == cuts - 1
        if last:
            both = [mul(under(g * masks[cut], k), x) for g, k, x in zip(grams, keys_t, xs)]
            ns, xs = [b[:half] for b in both], [b[half:] for b in both]
        else:
            ns = [mul(g * masks[cut], x) for g, x in zip(grams, xs)]
        tick()
        pairs = [mul(under(q, x), q) for q, x in zip(ns, xs)]
        tick()
        xs = [x - p[half:] for x, p in zip(xs, pairs)]
        xs = [x + mul(x, p[:half]) for x, p in zip(xs, pairs)]
    if cuts == 1:
        tick()
        xs = [mul(k, x) for k, x in zip(keys_t, xs)]
    tick()
    first = [dot(x[:, :half], r[:half]) for x, r in zip(xs, rights)]
    second = [dot(x[:, half:], r[half:]) for x, r in zip(xs, rights)]
    tick()
    dim = keys_t[0].shape[0]
    out = [a + b - dot(b[:, dim:].astype(BF16), a.astype(BF16)) for a, b in zip(first, second)]
    tick()
    return out


def kernel(
    n, tp, groups, per, dim,
    prompt, key_w, value_w, beta_w, bias, decay, query, gain,
    state_out, read_out,
    feat, weights, total, projected, beta_buf, bias_buf, decay_buf, query_buf, gain_buf,
    mask_buf, eye_buf, strength_buf, spans, partner_spans, joined, recv,
    ask_buf, row_stage, read_stage, read_recv,
    in_sem, beta_sem, feat_send, feat_recv, weight_sem, pair_send, pair_recv,
    map_send, map_recv, row_send, row_got, read_send, read_got,
):
    me = lax.axis_index("sp")
    core = lax.axis_index("tp")
    seg, part = prompt.shape[1], prompt.shape[2]
    wide = per * dim
    full = seg * n
    stride = n // groups
    half = groups // 2
    parity = lax.rem(me, 2)
    mine = me // stride
    chunk = min(part, 1024)

    order = list(range(half // 2, half)) + list(range(half // 2 - 1, -1, -1))
    sequence = [(0, order[0])]
    for j in range(half):
        if j + 1 < half:
            sequence.append((0, order[j + 1]))
        sequence.append((1, order[j]))
    plan = [range(1)] + [range(k, k + 2) for k in range(1, groups - 1, 2)] + [range(groups - 1, groups)]
    steps = len(plan)
    early = 1 + len(plan[1])

    def owner(g):
        return g * stride + (lax.rem(g, 2) if stride > 1 else 0)

    is_owner = me == owner(mine)

    def when_owner(work):
        if stride == 1:
            work()
        else:
            pl.when(is_owner)(work)

    def pair_at(j):
        pair = mine // 2
        if half & (half - 1):
            return lax.rem(pair + j, half)
        place = pair
        for bit in range(half.bit_length()):
            if j >> bit & 1:
                place += (1 - 2 * lax.rem(pair // 2**bit, 2)) * 2**bit
        return place

    def group_at(index):
        keep, j = sequence[index]
        return 2 * pair_at(j) + (parity if keep else 1 - parity)

    def features_of(d):
        return pl.ds(pl.multiple_of(lax.rem(core + d, tp) * part, part), part)

    def fetch_step(step, low, high):
        for d in range(low, high):
            for index in plan[step]:
                columns = pl.ds(pl.multiple_of(group_at(index) * wide, wide), wide)
                for j, w in enumerate((key_w, value_w)):
                    pltpu.make_async_copy(
                        w.at[features_of(d), columns], weights.at[index, d, j],
                        weight_sem.at[step, min(low, 1)],
                    ).start()

    def fetched(step, low, high):
        landed = weights.at[plan[step][0]:plan[step][-1] + 1, low:high]
        pltpu.make_async_copy(landed, landed, weight_sem.at[step, min(low, 1)]).wait()

    own_prompt = pltpu.make_async_copy(prompt.at[0], feat.at[0], in_sem.at[0])
    small = [
        pltpu.make_async_copy(src, dst, in_sem.at[1 + k])
        for k, (src, dst) in enumerate(
            ((bias, bias_buf), (decay, decay_buf), (query, query_buf), (gain, gain_buf))
        )
    ] + [
        pltpu.make_async_copy(beta_w.at[:, features_of(d)], beta_buf.at[d], beta_sem.at[d]) for d in range(tp)
    ]
    own_prompt.start()
    for copy in small:
        copy.start()
    fetch_step(0, 0, 1)
    fetch_step(1, 0, 1)

    barrier = pltpu.get_barrier_semaphore()
    for d in range(1, tp):
        pl.semaphore_signal(barrier, inc=1, device_id={"tp": lax.rem(core + d, tp)}, device_id_type=MESH)
    for d in range(1, n):
        pl.semaphore_signal(barrier, inc=1, device_id={"sp": lax.rem(me + d, n)}, device_id_type=MESH)
    masks, eye = cut_masks(seg // 2)
    for k, mask in enumerate(masks):
        mask_buf[k] = mask
    eye_buf[...] = eye
    own_prompt.wait()
    pl.semaphore_wait(barrier, n - 1 + tp - 1)

    def feature_copy(d):
        return pltpu.make_async_remote_copy(
            src_ref=feat.at[0], dst_ref=feat.at[tp - d],
            send_sem=feat_send.at[d - 1], recv_sem=feat_recv.at[tp - d],
            device_id={"tp": lax.rem(core + d, tp)}, device_id_type=MESH,
        )

    for d in range(1, tp):
        feature_copy(d).start()
    fetch_step(0, 1, tp)
    fetch_step(1, 1, tp)

    def begin(step):
        fetched(step, 0, 1)
        for index in plan[step]:
            for j in range(2):
                total[index, j] = dot(feat[0], weights[index, 0, j])

    for copy in small:
        copy.wait()
    before = dot(feat[0], beta_buf[0], ((1,), (1,)))
    begin(0)
    begin(1)
    if steps > 2:
        fetch_step(2, 0, tp)
    fetched(0, 1, tp)
    for d in range(1, tp):
        feature_copy(tp - d).wait_recv()
    for d in range(1, tp):
        before += dot(feat[d], beta_buf[d], ((1,), (1,)))
    strength_buf[...] = jax.nn.sigmoid(before + bias_buf[...])
    for index in plan[0]:
        for j in range(2):
            acc = total[index, j]
            for d in range(1, tp):
                acc += dot(feat[d], weights[index, d, j])
            projected[index, j] = acc.astype(BF16)

    def pair_copy(index, j):
        return pltpu.make_async_remote_copy(
            src_ref=spans.at[index], dst_ref=partner_spans.at[j],
            send_sem=pair_send, recv_sem=pair_recv.at[j],
            device_id={"sp": me + 1 - 2 * parity}, device_id_type=MESH,
        )

    def map_copy(j, slot):
        return pltpu.make_async_remote_copy(
            src_ref=joined.at[j], dst_ref=recv.at[slot],
            send_sem=map_send, recv_sem=map_recv.at[slot],
            device_id={"sp": owner(2 * pair_at(j) + parity)}, device_id_type=MESH,
        )

    def is_away(j):
        return owner(2 * pair_at(j) + parity) != me

    def pass_on(step):
        for index in plan[step]:
            keep, j = sequence[index]
            if not keep:
                pair_copy(index, j).start()
        for index in plan[step]:
            keep, j = sequence[index]
            if keep:
                pair_copy(index, j).wait_recv()
                for h in range(per):
                    ours, theirs = spans[index, h], partner_spans[j, h]
                    early = jnp.where(parity == 1, theirs, ours)
                    late = jnp.where(parity == 1, ours, theirs)
                    both = early.astype(F32) + late.astype(F32) - dot(late[:, dim:], early)
                    joined[j, h] = both.astype(BF16)
                if j or stride > 1:
                    @pl.when(is_away(j))
                    def _():
                        map_copy(j, me // 2).start()

    def projection(step):
        for index in plan[step]:
            for j in range(2):
                acc = total[index, j] if index < early else None
                for d in range(1 if index < early else 0, tp):
                    for low in range(0, part, chunk):
                        piece = dot(
                            feat[d, :, low:low + chunk], weights[index, d, j, low:low + chunk, :]
                        )
                        acc = piece if acc is None else acc + piece
                        if d == tp - 1 and low + chunk == part:
                            projected[index, j] = acc.astype(BF16)
                        yield

    ticks = 2 + 3 * len(masks) + 1
    for step in range(steps):
        if step > 0:
            pass_on(step - 1)
        if 2 < step + 2 < steps:
            fetch_step(step + 2, 0, tp)
        filler, units = iter(()), 0
        if step + 1 < steps:
            skip = 1 if step == 0 else 0
            units = len(plan[step + 1]) * 2 * (tp - skip) * (part // chunk)
            fetched(step + 1, skip, tp)
            filler = projection(step + 1)
        done = [0, 0]

        def tick():
            done[0] += 1
            while done[1] * ticks < done[0] * units:
                done[1] += 1
                next(filler, None)

        strengths = strength_buf[...]
        rates = decay_buf[...]
        lane = lax.broadcasted_iota(jnp.int32, strengths.shape, 1)
        rest = full - 1 - me * seg - lax.broadcasted_iota(jnp.int32, (seg, 1), 0)
        rest = rest.astype(F32) * (1.0 / full)
        heads = []
        for index in plan[step]:
            keys, values = projected[index, 0], projected[index, 1]
            for h in range(per):
                head = group_at(index) * per + h
                strength = jnp.sum(jnp.where(lane == head, strengths, 0.0), axis=1, keepdims=True)
                rate = jnp.sum(jnp.where(lane[:1] == head, rates, 0.0), axis=1, keepdims=True)
                fade = jnp.exp(-rate * rest)
                cols = slice(h * dim, (h + 1) * dim)
                heads.append((keys[:, cols], values[:, cols], strength, fade))
        results = span(heads, mask_buf, eye_buf, tick)
        for _ in filler:
            pass
        for k, result in enumerate(results):
            spans[plan[step][0] + k // per, k % per] = result.astype(BF16)
    rows = dim // n

    def row_copy(q):
        return pltpu.make_async_remote_copy(
            src_ref=row_stage.at[q], dst_ref=state_out.at[0, pl.ds(mine * per, per)],
            send_sem=row_send, recv_sem=row_got,
            device_id={"sp": q}, device_id_type=MESH,
        )

    def read_copy(q):
        return pltpu.make_async_remote_copy(
            src_ref=read_stage.at[q], dst_ref=read_recv.at[mine],
            send_sem=read_send, recv_sem=read_got,
            device_id={"sp": q}, device_id_type=MESH,
        )

    unit = query_buf[0].astype(F32)
    unit = unit * lax.rsqrt(jnp.sum(unit * unit, axis=1, keepdims=True) + 1.0)
    which = lax.broadcasted_iota(jnp.int32, unit.shape, 0)
    for h in range(per):
        row = jnp.sum(jnp.where(which == mine * per + h, unit, 0.0), axis=0, keepdims=True)
        ask_buf[h] = jnp.broadcast_to(row, (dim, dim)).T
    pass_on(steps - 1)
    recv[me // 2] = joined[0]

    def finish():
        def arrive(p):
            @pl.when(p != me // 2)
            def _():
                map_copy(0, p).wait_recv()

        arrive(0)
        states = [recv[0, h, :, :dim].astype(F32) for h in range(per)]
        for p in range(1, n // 2):
            arrive(p)
            for h in range(per):
                write, drop = recv[p, h, :, :dim].astype(F32), recv[p, h, :, dim:]
                high = states[h].astype(BF16)
                low = (states[h] - high.astype(F32)).astype(BF16)
                states[h] = states[h] + (write - dot(drop, high) - dot(drop, low))
        for h in range(per):
            cast = states[h].astype(BF16)
            for q in range(n):
                row_stage[q, h] = cast[q * rows:(q + 1) * rows]
        for d in range(n - 1, 0, -1):
            row_copy(lax.rem(me + d, n)).start()
        for h in range(per):
            raw = jnp.sum(ask_buf[h] * states[h], axis=0, keepdims=True)
            raw = raw * lax.rsqrt(jnp.mean(raw * raw, axis=1, keepdims=True) + 0.05) * gain_buf[...]
            for q in range(n):
                read_stage[q, h:h + 1] = raw
        for d in range(1, n):
            read_copy(lax.rem(me + d, n)).start()
        state_out[0, pl.ds(mine * per, per)] = row_stage[me]
        read_recv[mine] = read_stage[0]

    when_owner(finish)

    def wait_all(count):
        rows_in, reads_in = state_out.at[0, :count * per], read_recv.at[:count]
        pltpu.make_async_copy(rows_in, rows_in, row_got).wait()
        pltpu.make_async_copy(reads_in, reads_in, read_got).wait()

    def wait_sent():
        for done, sem in ((row_stage.at[1:], row_send), (read_stage.at[1:], read_send)):
            pltpu.make_async_copy(done, done, sem).wait()

    def wait_maps(low):
        if low < half:
            done = joined.at[low:]
            pltpu.make_async_copy(done, done, map_send).wait()

    if stride == 1:
        wait_all(groups - 1)
    else:
        pl.when(is_owner)(lambda: wait_all(groups - 1))
        pl.when(jnp.logical_not(is_owner))(lambda: wait_all(groups))
    for g in range(groups):
        read_out[0, g * per:(g + 1) * per] = read_recv[g]
    for d in range(1, tp):
        feature_copy(d).wait_send()
    pltpu.make_async_copy(partner_spans, partner_spans, pair_send).wait()
    if stride == 1:
        wait_maps(1)
    else:
        pl.when(is_owner)(lambda: wait_maps(1))
        pl.when(jnp.logical_not(is_owner))(lambda: wait_maps(0))
    when_owner(wait_sent)


def deliver(state, read, state_out, read_out, sem):
    copies = [
        pltpu.make_async_copy(src, dst, sem.at[k])
        for k, (src, dst) in enumerate(((state, state_out), (read, read_out)))
    ]
    for copy in copies:
        copy.start()
    for copy in copies:
        copy.wait()


def solution(mesh):
    n, tp = mesh.shape["sp"], mesh.shape["tp"]

    def shards(prompt, key_w, value_w, beta_w, bias, decay, query, gain):
        seg, part = prompt.shape[1:]
        depth = key_w.shape[0]
        heads = beta_w.shape[1]
        dim = key_w.shape[1] // heads
        per = max(1, heads // n)
        groups = heads // per
        wide = per * dim
        rows = dim // n
        block = seg // 2
        cuts = len(bounds(block))
        dma = pltpu.SemaphoreType.DMA
        vmem = pl.BlockSpec(memory_space=pltpu.VMEM)
        hbm = pl.BlockSpec(memory_space=pl.ANY)
        half = groups // 2
        found = pl.pallas_call(
            functools.partial(kernel, n, tp, groups, per, dim),
            out_shape=(
                pltpu.VMEM((1, heads, rows, dim), BF16),
                pltpu.VMEM((1, heads, dim), F32),
            ),
            in_specs=[hbm] * 8,
            out_specs=(vmem, vmem),
            scratch_shapes=[
                pltpu.VMEM((tp, seg, part), BF16),
                pltpu.VMEM((groups, tp, 2, part, wide), BF16),
                pltpu.VMEM((3, 2, seg, wide), F32),
                pltpu.VMEM((groups, 2, seg, wide), BF16),
                pltpu.VMEM((tp, heads, part), BF16),
                pltpu.VMEM((1, heads), F32),
                pltpu.VMEM((1, heads), F32),
                pltpu.VMEM((1, heads, dim), BF16),
                pltpu.VMEM((1, dim), F32),
                pltpu.VMEM((cuts, block, seg), BF16),
                pltpu.VMEM((block, seg), BF16),
                pltpu.VMEM((seg, heads), F32),
                pltpu.VMEM((groups, per, dim, 2 * dim), BF16),
                pltpu.VMEM((half, per, dim, 2 * dim), BF16),
                pltpu.VMEM((half, per, dim, 2 * dim), BF16),
                pltpu.VMEM((n // 2, per, dim, 2 * dim), BF16),
                pltpu.VMEM((per, dim, dim), F32),
                pltpu.VMEM((n, per, rows, dim), BF16),
                pltpu.VMEM((n, per, dim), F32),
                pltpu.VMEM((groups, per, dim), F32),
                dma((5,)),
                dma((tp,)),
                dma((tp - 1,)),
                dma((tp,)),
                dma((groups // 2 + 1, 2)),
                pltpu.SemaphoreType.DMA,
                dma((half,)),
                pltpu.SemaphoreType.DMA,
                dma((n // 2,)),
                pltpu.SemaphoreType.DMA,
                pltpu.SemaphoreType.DMA,
                pltpu.SemaphoreType.DMA,
                pltpu.SemaphoreType.DMA,
            ],
            compiler_params=pltpu.CompilerParams(
                collective_id=0, has_side_effects=True, vmem_limit_bytes=60 * 2**20
            ),
        )(
            prompt, key_w, value_w, beta_w.T, bias.reshape(1, heads), decay.reshape(1, heads),
            query, gain.reshape(1, dim),
        )
        return pl.pallas_call(
            deliver,
            out_shape=tuple(jax.ShapeDtypeStruct(x.shape, x.dtype) for x in found),
            in_specs=[vmem] * 2,
            out_specs=(hbm, hbm),
            scratch_shapes=[dma((2,))],
        )(*(pltpu.with_memory_space_constraint(x, pltpu.VMEM) for x in found))

    return jax.shard_map(
        shards,
        mesh=mesh,
        in_specs=(
            P("gr", "sp", "tp"),
            P(None, "tp"),
            P(None, "tp"),
            P(None, "tp"),
            P("tp"),
            P("tp"),
            P("gr", "tp", None),
            P(),
        ),
        out_specs=(P("gr", "tp", "sp", None), P("gr", "tp", None)),
        check_vma=False,
    )
```

```python
import functools

import jax
import jax.numpy as jnp
from jax import lax
from jax.experimental import pallas as pl
from jax.experimental.pallas import tpu as pltpu
from jax.sharding import PartitionSpec as P

MESH = pl.DeviceIdType.MESH
F32 = jnp.float32
BF16 = jnp.bfloat16


def dot(left, right, contract=((1,), (0,))):
    return lax.dot_general(left, right, (contract, ((), ())), preferred_element_type=F32)


def bounds(size):
    levels = (size - 1).bit_length()
    cuts = [0, min(3, levels)]
    while cuts[-1] < levels:
        cuts.append(min(cuts[-1] + 2, levels))
    return tuple(zip(cuts[:-1], cuts[1:]))


def cut_masks(size):
    row = lax.broadcasted_iota(jnp.int32, (size, 2 * size), 0)
    col = lax.rem(lax.broadcasted_iota(jnp.int32, (size, 2 * size), 1), size)
    masks = []
    for low, high in bounds(size):
        together = (row >> high) == (col >> high)
        apart = (row >> low) != (col >> low)
        masks.append((together & apart & (row > col)).astype(F32).astype(BF16))
    return masks, (row == col).astype(F32).astype(BF16)


def spread(x):
    size = x.shape[1] // 2
    zero = jnp.zeros((x.shape[0], size), x.dtype)
    return jnp.concatenate(
        [jnp.concatenate([x[:, :size], zero], axis=1), jnp.concatenate([zero, x[:, size:]], axis=1)], axis=0
    )


def under(x, y):
    return jnp.concatenate([x, y], axis=0)


def mul(x, y):
    return dot(x, spread(y)).astype(BF16)


def span(heads, masks, eye, tick):
    keys_t, rights, grams = [], [], []
    for key, value, strength, fade in heads:
        key = key.astype(F32)
        key = key * lax.rsqrt(jnp.sum(key * key, axis=1, keepdims=True) + 1.0)
        weighted = (key * strength).astype(BF16)
        value = (value.astype(F32) * (strength * fade)).astype(BF16)
        key_t = key.astype(BF16).T
        half = weighted.shape[0] // 2
        keys_t.append(key_t)
        rights.append(jnp.concatenate([value, weighted], axis=1))
        grams.append(mul(jnp.concatenate([weighted[:half], weighted[half:]], axis=1), key_t))
    cuts = masks.shape[0]
    tick()
    ns = [g * masks[0] for g in grams]
    squares = [mul(x, x) for x in ns]
    tick()
    xs = [eye[...] - x for x in ns]
    pairs = [mul(under(q, x), q) for q, x in zip(squares, xs)]
    tick()
    xs = [x + p[half:] for x, p in zip(xs, pairs)]
    xs = [x + mul(x, p[:half]) for x, p in zip(xs, pairs)]
    for cut in range(1, cuts):
        tick()
        last = cut == cuts - 1
        if last:
            both = [mul(under(g * masks[cut], k), x) for g, k, x in zip(grams, keys_t, xs)]
            ns, xs = [b[:half] for b in both], [b[half:] for b in both]
        else:
            ns = [mul(g * masks[cut], x) for g, x in zip(grams, xs)]
        tick()
        pairs = [mul(under(q, x), q) for q, x in zip(ns, xs)]
        tick()
        xs = [x - p[half:] for x, p in zip(xs, pairs)]
        xs = [x + mul(x, p[:half]) for x, p in zip(xs, pairs)]
    if cuts == 1:
        tick()
        xs = [mul(k, x) for k, x in zip(keys_t, xs)]
    tick()
    first = [dot(x[:, :half], r[:half]) for x, r in zip(xs, rights)]
    second = [dot(x[:, half:], r[half:]) for x, r in zip(xs, rights)]
    tick()
    dim = keys_t[0].shape[0]
    out = [a + b - dot(b[:, dim:].astype(BF16), a.astype(BF16)) for a, b in zip(first, second)]
    tick()
    return out


def kernel(
    n, tp, groups, per, dim,
    prompt, key_w, value_w, beta_w, bias, decay, query, gain,
    state_out, read_out,
    feat, weights, total, projected, beta_buf, bias_buf, decay_buf, query_buf, gain_buf,
    mask_buf, eye_buf, strength_buf, spans, partner_spans, joined, recv,
    ask_buf, row_stage, read_stage, read_recv,
    in_sem, beta_sem, feat_send, feat_recv, weight_sem, pair_send, pair_recv,
    map_send, map_recv, row_send, row_got, read_send, read_got,
):
    me = lax.axis_index("sp")
    core = lax.axis_index("tp")
    seg, part = prompt.shape[1], prompt.shape[2]
    wide = per * dim
    full = seg * n
    stride = n // groups
    half = groups // 2
    parity = lax.rem(me, 2)
    mine = me // stride
    chunk = min(part, 1024)

    order = list(range(half // 2, half)) + list(range(half // 2 - 1, -1, -1))
    sequence = [(0, order[0])]
    for j in range(half):
        if j + 1 < half:
            sequence.append((0, order[j + 1]))
        sequence.append((1, order[j]))
    plan = [range(1)] + [range(k, k + 2) for k in range(1, groups - 1, 2)] + [range(groups - 1, groups)]
    steps = len(plan)
    early = 1 + len(plan[1])

    def owner(g):
        return g * stride + (lax.rem(g, 2) if stride > 1 else 0)

    is_owner = me == owner(mine)

    def when_owner(work):
        if stride == 1:
            work()
        else:
            pl.when(is_owner)(work)

    def pair_at(j):
        pair = mine // 2
        if half & (half - 1):
            return lax.rem(pair + j, half)
        place = pair
        for bit in range(half.bit_length()):
            if j >> bit & 1:
                place += (1 - 2 * lax.rem(pair // 2**bit, 2)) * 2**bit
        return place

    def group_at(index):
        keep, j = sequence[index]
        return 2 * pair_at(j) + (parity if keep else 1 - parity)

    def features_of(d):
        return pl.ds(pl.multiple_of(lax.rem(core + d, tp) * part, part), part)

    def fetch_step(step, low, high):
        for d in range(low, high):
            for index in plan[step]:
                columns = pl.ds(pl.multiple_of(group_at(index) * wide, wide), wide)
                for j, w in enumerate((key_w, value_w)):
                    pltpu.make_async_copy(
                        w.at[features_of(d), columns], weights.at[index, d, j],
                        weight_sem.at[step, min(low, 1)],
                    ).start()

    def fetched(step, low, high):
        landed = weights.at[plan[step][0]:plan[step][-1] + 1, low:high]
        pltpu.make_async_copy(landed, landed, weight_sem.at[step, min(low, 1)]).wait()

    own_prompt = pltpu.make_async_copy(prompt.at[0], feat.at[0], in_sem.at[0])
    small = [
        pltpu.make_async_copy(src, dst, in_sem.at[1 + k])
        for k, (src, dst) in enumerate(
            ((bias, bias_buf), (decay, decay_buf), (query, query_buf), (gain, gain_buf))
        )
    ] + [
        pltpu.make_async_copy(beta_w.at[:, features_of(d)], beta_buf.at[d], beta_sem.at[d]) for d in range(tp)
    ]
    own_prompt.start()
    for copy in small:
        copy.start()
    fetch_step(0, 0, 1)
    fetch_step(1, 0, 1)

    barrier = pltpu.get_barrier_semaphore()
    for d in range(1, tp):
        pl.semaphore_signal(barrier, inc=1, device_id={"tp": lax.rem(core + d, tp)}, device_id_type=MESH)
    for d in range(1, n):
        pl.semaphore_signal(barrier, inc=1, device_id={"sp": lax.rem(me + d, n)}, device_id_type=MESH)
    masks, eye = cut_masks(seg // 2)
    for k, mask in enumerate(masks):
        mask_buf[k] = mask
    eye_buf[...] = eye
    own_prompt.wait()
    pl.semaphore_wait(barrier, n - 1 + tp - 1)

    def feature_copy(d):
        return pltpu.make_async_remote_copy(
            src_ref=feat.at[0], dst_ref=feat.at[tp - d],
            send_sem=feat_send.at[d - 1], recv_sem=feat_recv.at[tp - d],
            device_id={"tp": lax.rem(core + d, tp)}, device_id_type=MESH,
        )

    for d in range(1, tp):
        feature_copy(d).start()

    def begin(step):
        fetched(step, 0, 1)
        for index in plan[step]:
            for j in range(2):
                total[index, j] = dot(feat[0], weights[index, 0, j])

    fetch_step(0, 1, tp)
    begin(0)
    fetch_step(1, 1, tp)
    begin(1)
    for copy in small:
        copy.wait()
    fetched(0, 1, tp)
    fetched(1, 1, tp)
    if steps > 2:
        fetch_step(2, 0, tp)
    for d in range(1, tp):
        feature_copy(tp - d).wait_recv()
    before = dot(feat[0], beta_buf[0], ((1,), (1,)))
    for d in range(1, tp):
        before += dot(feat[d], beta_buf[d], ((1,), (1,)))
    strength_buf[...] = jax.nn.sigmoid(before + bias_buf[...])
    for index in plan[0]:
        for j in range(2):
            acc = total[index, j]
            for d in range(1, tp):
                acc += dot(feat[d], weights[index, d, j])
            projected[index, j] = acc.astype(BF16)

    def pair_copy(index, j):
        return pltpu.make_async_remote_copy(
            src_ref=spans.at[index], dst_ref=partner_spans.at[j],
            send_sem=pair_send, recv_sem=pair_recv.at[j],
            device_id={"sp": me + 1 - 2 * parity}, device_id_type=MESH,
        )

    def map_copy(j, slot):
        return pltpu.make_async_remote_copy(
            src_ref=joined.at[j], dst_ref=recv.at[slot],
            send_sem=map_send, recv_sem=map_recv.at[slot],
            device_id={"sp": owner(2 * pair_at(j) + parity)}, device_id_type=MESH,
        )

    def is_away(j):
        return owner(2 * pair_at(j) + parity) != me

    def pass_on(step):
        for index in plan[step]:
            keep, j = sequence[index]
            if not keep:
                pair_copy(index, j).start()

    def join(step):
        for index in plan[step]:
            keep, j = sequence[index]
            if keep:
                pair_copy(index, j).wait_recv()
                for h in range(per):
                    ours, theirs = spans[index, h], partner_spans[j, h]
                    early = jnp.where(parity == 1, theirs, ours)
                    late = jnp.where(parity == 1, ours, theirs)
                    both = early.astype(F32) + late.astype(F32) - dot(late[:, dim:], early)
                    joined[j, h] = both.astype(BF16)
                if j or stride > 1:
                    @pl.when(is_away(j))
                    def _():
                        map_copy(j, me // 2).start()

    def projection(step):
        for index in plan[step]:
            for j in range(2):
                acc = total[index, j] if index < early else None
                for d in range(1 if index < early else 0, tp):
                    for low in range(0, part, chunk):
                        piece = dot(
                            feat[d, :, low:low + chunk], weights[index, d, j, low:low + chunk, :]
                        )
                        acc = piece if acc is None else acc + piece
                        if d == tp - 1 and low + chunk == part:
                            projected[index, j] = acc.astype(BF16)
                        yield

    ticks = 2 + 3 * len(masks) + 1
    for step in range(steps):
        if step > 0:
            pass_on(step - 1)
        if 2 < step + 2 < steps:
            fetch_step(step + 2, 0, tp)
        filler, units = iter(()), 0
        if step + 1 < steps:
            skip = 1 if step == 0 else 0
            units = len(plan[step + 1]) * 2 * (tp - skip) * (part // chunk)
            if step > 0:
                fetched(step + 1, skip, tp)
            filler = projection(step + 1)
        done = [0, 0]
        when = 0
        if step == 2:
            when = 0
        elif step == steps - 1:
            when = 0
        if step > 0 and when == 0:
            join(step - 1)

        def tick():
            done[0] += 1
            if step > 0 and done[0] == when:
                join(step - 1)
            while done[1] * ticks < done[0] * units:
                done[1] += 1
                next(filler, None)

        strengths = strength_buf[...]
        rates = decay_buf[...]
        lane = lax.broadcasted_iota(jnp.int32, strengths.shape, 1)
        rest = full - 1 - me * seg - lax.broadcasted_iota(jnp.int32, (seg, 1), 0)
        rest = rest.astype(F32) * (1.0 / full)
        heads = []
        for index in plan[step]:
            keys, values = projected[index, 0], projected[index, 1]
            for h in range(per):
                head = group_at(index) * per + h
                strength = jnp.sum(jnp.where(lane == head, strengths, 0.0), axis=1, keepdims=True)
                rate = jnp.sum(jnp.where(lane[:1] == head, rates, 0.0), axis=1, keepdims=True)
                fade = jnp.exp(-rate * rest)
                cols = slice(h * dim, (h + 1) * dim)
                heads.append((keys[:, cols], values[:, cols], strength, fade))
        results = span(heads, mask_buf, eye_buf, tick)
        for _ in filler:
            pass
        for k, result in enumerate(results):
            spans[plan[step][0] + k // per, k % per] = result.astype(BF16)
    rows = dim // n

    def row_copy(q):
        return pltpu.make_async_remote_copy(
            src_ref=row_stage.at[q], dst_ref=state_out.at[0, pl.ds(mine * per, per)],
            send_sem=row_send, recv_sem=row_got,
            device_id={"sp": q}, device_id_type=MESH,
        )

    def read_copy(q):
        return pltpu.make_async_remote_copy(
            src_ref=read_stage.at[q], dst_ref=read_recv.at[mine],
            send_sem=read_send, recv_sem=read_got,
            device_id={"sp": q}, device_id_type=MESH,
        )

    unit = query_buf[0].astype(F32)
    unit = unit * lax.rsqrt(jnp.sum(unit * unit, axis=1, keepdims=True) + 1.0)
    which = lax.broadcasted_iota(jnp.int32, unit.shape, 0)
    for h in range(per):
        row = jnp.sum(jnp.where(which == mine * per + h, unit, 0.0), axis=0, keepdims=True)
        ask_buf[h] = jnp.broadcast_to(row, (dim, dim)).T
    join(steps - 1)
    recv[me // 2] = joined[0]

    def finish():
        def arrive(p):
            @pl.when(p != me // 2)
            def _():
                map_copy(0, p).wait_recv()

        arrive(0)
        states = [recv[0, h, :, :dim].astype(F32) for h in range(per)]
        for p in range(1, n // 2):
            arrive(p)
            for h in range(per):
                write, drop = recv[p, h, :, :dim].astype(F32), recv[p, h, :, dim:]
                high = states[h].astype(BF16)
                low = (states[h] - high.astype(F32)).astype(BF16)
                states[h] = states[h] + (write - dot(drop, high) - dot(drop, low))
        for h in range(per):
            cast = states[h].astype(BF16)
            for q in range(n):
                row_stage[q, h] = cast[q * rows:(q + 1) * rows]
        for d in range(n - 1, 0, -1):
            row_copy(lax.rem(me + d, n)).start()
        for h in range(per):
            raw = jnp.sum(ask_buf[h] * states[h], axis=0, keepdims=True)
            raw = raw * lax.rsqrt(jnp.mean(raw * raw, axis=1, keepdims=True) + 0.05) * gain_buf[...]
            for q in range(n):
                read_stage[q, h:h + 1] = raw
        for d in range(1, n):
            read_copy(lax.rem(me + d, n)).start()
        state_out[0, pl.ds(mine * per, per)] = row_stage[me]
        read_recv[mine] = read_stage[0]

    when_owner(finish)

    def wait_all(count):
        rows_in, reads_in = state_out.at[0, :count * per], read_recv.at[:count]
        pltpu.make_async_copy(rows_in, rows_in, row_got).wait()
        pltpu.make_async_copy(reads_in, reads_in, read_got).wait()

    def wait_sent():
        for done, sem in ((row_stage.at[1:], row_send), (read_stage.at[1:], read_send)):
            pltpu.make_async_copy(done, done, sem).wait()

    def wait_maps(low):
        if low < half:
            done = joined.at[low:]
            pltpu.make_async_copy(done, done, map_send).wait()

    if stride == 1:
        wait_all(groups - 1)
    else:
        pl.when(is_owner)(lambda: wait_all(groups - 1))
        pl.when(jnp.logical_not(is_owner))(lambda: wait_all(groups))
    for g in range(groups):
        read_out[0, g * per:(g + 1) * per] = read_recv[g]
    for d in range(1, tp):
        feature_copy(d).wait_send()
    pltpu.make_async_copy(partner_spans, partner_spans, pair_send).wait()
    if stride == 1:
        wait_maps(1)
    else:
        pl.when(is_owner)(lambda: wait_maps(1))
        pl.when(jnp.logical_not(is_owner))(lambda: wait_maps(0))
    when_owner(wait_sent)


def deliver(state, read, state_out, read_out, sem):
    copies = [
        pltpu.make_async_copy(src, dst, sem.at[k])
        for k, (src, dst) in enumerate(((state, state_out), (read, read_out)))
    ]
    for copy in copies:
        copy.start()
    for copy in copies:
        copy.wait()


def solution(mesh):
    n, tp = mesh.shape["sp"], mesh.shape["tp"]

    def shards(prompt, key_w, value_w, beta_w, bias, decay, query, gain):
        seg, part = prompt.shape[1:]
        depth = key_w.shape[0]
        heads = beta_w.shape[1]
        dim = key_w.shape[1] // heads
        per = max(1, heads // n)
        groups = heads // per
        wide = per * dim
        rows = dim // n
        block = seg // 2
        cuts = len(bounds(block))
        dma = pltpu.SemaphoreType.DMA
        vmem = pl.BlockSpec(memory_space=pltpu.VMEM)
        hbm = pl.BlockSpec(memory_space=pl.ANY)
        half = groups // 2
        found = pl.pallas_call(
            functools.partial(kernel, n, tp, groups, per, dim),
            out_shape=(
                pltpu.VMEM((1, heads, rows, dim), BF16),
                pltpu.VMEM((1, heads, dim), F32),
            ),
            in_specs=[hbm] * 8,
            out_specs=(vmem, vmem),
            scratch_shapes=[
                pltpu.VMEM((tp, seg, part), BF16),
                pltpu.VMEM((groups, tp, 2, part, wide), BF16),
                pltpu.VMEM((3, 2, seg, wide), F32),
                pltpu.VMEM((groups, 2, seg, wide), BF16),
                pltpu.VMEM((tp, heads, part), BF16),
                pltpu.VMEM((1, heads), F32),
                pltpu.VMEM((1, heads), F32),
                pltpu.VMEM((1, heads, dim), BF16),
                pltpu.VMEM((1, dim), F32),
                pltpu.VMEM((cuts, block, seg), BF16),
                pltpu.VMEM((block, seg), BF16),
                pltpu.VMEM((seg, heads), F32),
                pltpu.VMEM((groups, per, dim, 2 * dim), BF16),
                pltpu.VMEM((half, per, dim, 2 * dim), BF16),
                pltpu.VMEM((half, per, dim, 2 * dim), BF16),
                pltpu.VMEM((n // 2, per, dim, 2 * dim), BF16),
                pltpu.VMEM((per, dim, dim), F32),
                pltpu.VMEM((n, per, rows, dim), BF16),
                pltpu.VMEM((n, per, dim), F32),
                pltpu.VMEM((groups, per, dim), F32),
                dma((5,)),
                dma((tp,)),
                dma((tp - 1,)),
                dma((tp,)),
                dma((groups // 2 + 1, 2)),
                pltpu.SemaphoreType.DMA,
                dma((half,)),
                pltpu.SemaphoreType.DMA,
                dma((n // 2,)),
                pltpu.SemaphoreType.DMA,
                pltpu.SemaphoreType.DMA,
                pltpu.SemaphoreType.DMA,
                pltpu.SemaphoreType.DMA,
            ],
            compiler_params=pltpu.CompilerParams(
                collective_id=0, has_side_effects=True, vmem_limit_bytes=60 * 2**20
            ),
        )(
            prompt, key_w, value_w, beta_w.T, bias.reshape(1, heads), decay.reshape(1, heads),
            query, gain.reshape(1, dim),
        )
        return pl.pallas_call(
            deliver,
            out_shape=tuple(jax.ShapeDtypeStruct(x.shape, x.dtype) for x in found),
            in_specs=[vmem] * 2,
            out_specs=(hbm, hbm),
            scratch_shapes=[dma((2,))],
        )(*(pltpu.with_memory_space_constraint(x, pltpu.VMEM) for x in found))

    return jax.shard_map(
        shards,
        mesh=mesh,
        in_specs=(
            P("gr", "sp", "tp"),
            P(None, "tp"),
            P(None, "tp"),
            P(None, "tp"),
            P("tp"),
            P("tp"),
            P("gr", "tp", None),
            P(),
        ),
        out_specs=(P("gr", "tp", "sp", None), P("gr", "tp", None)),
        check_vma=False,
    )
```

```python
import functools

import jax
import jax.numpy as jnp
from jax import lax
from jax.experimental import pallas as pl
from jax.experimental.pallas import tpu as pltpu
from jax.sharding import PartitionSpec as P

MESH = pl.DeviceIdType.MESH
F32 = jnp.float32
BF16 = jnp.bfloat16


def dot(left, right, contract=((1,), (0,))):
    return lax.dot_general(left, right, (contract, ((), ())), preferred_element_type=F32)


def bounds(size):
    levels = (size - 1).bit_length()
    cuts = [0, min(3, levels)]
    while cuts[-1] < levels:
        cuts.append(min(cuts[-1] + 2, levels))
    return tuple(zip(cuts[:-1], cuts[1:]))


def cut_masks(size):
    row = lax.broadcasted_iota(jnp.int32, (size, 2 * size), 0)
    col = lax.rem(lax.broadcasted_iota(jnp.int32, (size, 2 * size), 1), size)
    masks = []
    for low, high in bounds(size):
        together = (row >> high) == (col >> high)
        apart = (row >> low) != (col >> low)
        masks.append((together & apart & (row > col)).astype(F32).astype(BF16))
    return masks, (row == col).astype(F32).astype(BF16)


def spread(x):
    size = x.shape[1] // 2
    zero = jnp.zeros((x.shape[0], size), x.dtype)
    return jnp.concatenate(
        [jnp.concatenate([x[:, :size], zero], axis=1), jnp.concatenate([zero, x[:, size:]], axis=1)], axis=0
    )


def under(x, y):
    return jnp.concatenate([x, y], axis=0)


def mul(x, y):
    return dot(x, spread(y)).astype(BF16)


def span(heads, masks, eye, tick):
    keys_t, rights, grams = [], [], []
    for key, value, strength, fade in heads:
        key = key.astype(F32)
        key = key * lax.rsqrt(jnp.sum(key * key, axis=1, keepdims=True) + 1.0)
        weighted = (key * strength).astype(BF16)
        value = (value.astype(F32) * (strength * fade)).astype(BF16)
        key_t = key.astype(BF16).T
        half = weighted.shape[0] // 2
        keys_t.append(key_t)
        rights.append(jnp.concatenate([value, weighted], axis=1))
        grams.append(mul(jnp.concatenate([weighted[:half], weighted[half:]], axis=1), key_t))
    cuts = masks.shape[0]
    tick()
    ns = [g * masks[0] for g in grams]
    squares = [mul(x, x) for x in ns]
    tick()
    xs = [eye[...] - x for x in ns]
    pairs = [mul(under(q, x), q) for q, x in zip(squares, xs)]
    tick()
    xs = [x + p[half:] for x, p in zip(xs, pairs)]
    xs = [x + mul(x, p[:half]) for x, p in zip(xs, pairs)]
    for cut in range(1, cuts):
        tick()
        last = cut == cuts - 1
        if last:
            both = [mul(under(g * masks[cut], k), x) for g, k, x in zip(grams, keys_t, xs)]
            ns, xs = [b[:half] for b in both], [b[half:] for b in both]
        else:
            ns = [mul(g * masks[cut], x) for g, x in zip(grams, xs)]
        tick()
        pairs = [mul(under(q, x), q) for q, x in zip(ns, xs)]
        tick()
        xs = [x - p[half:] for x, p in zip(xs, pairs)]
        xs = [x + mul(x, p[:half]) for x, p in zip(xs, pairs)]
    if cuts == 1:
        tick()
        xs = [mul(k, x) for k, x in zip(keys_t, xs)]
    tick()
    first = [dot(x[:, :half], r[:half]) for x, r in zip(xs, rights)]
    second = [dot(x[:, half:], r[half:]) for x, r in zip(xs, rights)]
    tick()
    dim = keys_t[0].shape[0]
    out = [a + b - dot(b[:, dim:].astype(BF16), a.astype(BF16)) for a, b in zip(first, second)]
    tick()
    return out


def kernel(
    n, tp, groups, per, dim,
    prompt, key_w, value_w, beta_w, bias, decay, query, gain,
    state_out, read_out,
    feat, weights, total, projected, beta_buf, bias_buf, decay_buf, query_buf, gain_buf,
    mask_buf, eye_buf, strength_buf, spans, partner_spans, joined, recv,
    ask_buf, row_stage, read_stage, read_recv,
    in_sem, beta_sem, feat_send, feat_recv, weight_sem, pair_send, pair_recv,
    map_send, map_recv, row_send, row_got, read_send, read_got,
):
    me = lax.axis_index("sp")
    core = lax.axis_index("tp")
    seg, part = prompt.shape[1], prompt.shape[2]
    wide = per * dim
    full = seg * n
    stride = n // groups
    half = groups // 2
    parity = lax.rem(me, 2)
    mine = me // stride
    chunk = min(part, 1024)

    order = list(range(half // 2, half)) + list(range(half // 2 - 1, -1, -1))
    sequence = [(0, order[0])]
    for j in range(half):
        if j + 1 < half:
            sequence.append((0, order[j + 1]))
        sequence.append((1, order[j]))
    plan = [range(1)] + [range(k, k + 2) for k in range(1, groups - 1, 2)] + [range(groups - 1, groups)]
    steps = len(plan)
    early = 1 + len(plan[1])

    def owner(g):
        return g * stride + (lax.rem(g, 2) if stride > 1 else 0)

    is_owner = me == owner(mine)

    def when_owner(work):
        if stride == 1:
            work()
        else:
            pl.when(is_owner)(work)

    def pair_at(j):
        pair = mine // 2
        if half & (half - 1):
            return lax.rem(pair + j, half)
        place = pair
        for bit in range(half.bit_length()):
            if j >> bit & 1:
                place += (1 - 2 * lax.rem(pair // 2**bit, 2)) * 2**bit
        return place

    def group_at(index):
        keep, j = sequence[index]
        return 2 * pair_at(j) + (parity if keep else 1 - parity)

    def features_of(d):
        return pl.ds(pl.multiple_of(lax.rem(core + d, tp) * part, part), part)

    def fetch_step(step, low, high):
        for d in range(low, high):
            for index in plan[step]:
                columns = pl.ds(pl.multiple_of(group_at(index) * wide, wide), wide)
                for j, w in enumerate((key_w, value_w)):
                    pltpu.make_async_copy(
                        w.at[features_of(d), columns], weights.at[index, d, j],
                        weight_sem.at[step, min(low, 1)],
                    ).start()

    def fetched(step, low, high):
        landed = weights.at[plan[step][0]:plan[step][-1] + 1, low:high]
        pltpu.make_async_copy(landed, landed, weight_sem.at[step, min(low, 1)]).wait()

    own_prompt = pltpu.make_async_copy(prompt.at[0], feat.at[0], in_sem.at[0])
    small = [
        pltpu.make_async_copy(src, dst, in_sem.at[1 + k])
        for k, (src, dst) in enumerate(
            ((bias, bias_buf), (decay, decay_buf), (query, query_buf), (gain, gain_buf))
        )
    ] + [
        pltpu.make_async_copy(beta_w.at[:, features_of(d)], beta_buf.at[d], beta_sem.at[d]) for d in range(tp)
    ]
    own_prompt.start()
    for copy in small:
        copy.start()
    fetch_step(0, 0, 1)
    fetch_step(1, 0, 1)

    partner_spans[:, :, :, dim:] = jnp.zeros((half, per, dim, dim), BF16)
    barrier = pltpu.get_barrier_semaphore()
    for d in range(1, tp):
        pl.semaphore_signal(barrier, inc=1, device_id={"tp": lax.rem(core + d, tp)}, device_id_type=MESH)
    for d in range(1, n):
        pl.semaphore_signal(barrier, inc=1, device_id={"sp": lax.rem(me + d, n)}, device_id_type=MESH)
    masks, eye = cut_masks(seg // 2)
    for k, mask in enumerate(masks):
        mask_buf[k] = mask
    eye_buf[...] = eye
    own_prompt.wait()
    pl.semaphore_wait(barrier, n - 1 + tp - 1)

    def feature_copy(d):
        return pltpu.make_async_remote_copy(
            src_ref=feat.at[0], dst_ref=feat.at[tp - d],
            send_sem=feat_send.at[d - 1], recv_sem=feat_recv.at[tp - d],
            device_id={"tp": lax.rem(core + d, tp)}, device_id_type=MESH,
        )

    for d in range(1, tp):
        feature_copy(d).start()

    def begin(step):
        fetched(step, 0, 1)
        for index in plan[step]:
            for j in range(2):
                total[index, j] = dot(feat[0], weights[index, 0, j])

    fetch_step(0, 1, tp)
    begin(0)
    fetch_step(1, 1, tp)
    begin(1)
    for copy in small:
        copy.wait()
    fetched(0, 1, tp)
    fetched(1, 1, tp)
    if steps > 2:
        fetch_step(2, 0, tp)
    for d in range(1, tp):
        feature_copy(tp - d).wait_recv()
    before = dot(feat[0], beta_buf[0], ((1,), (1,)))
    for d in range(1, tp):
        before += dot(feat[d], beta_buf[d], ((1,), (1,)))
    strength_buf[...] = jax.nn.sigmoid(before + bias_buf[...])
    for index in plan[0]:
        for j in range(2):
            acc = total[index, j]
            for d in range(1, tp):
                acc += dot(feat[d], weights[index, d, j])
            projected[index, j] = acc.astype(BF16)

    def pair_copy(index, j, last=2 * dim):
        return pltpu.make_async_remote_copy(
            src_ref=spans.at[index, :, :, :last], dst_ref=partner_spans.at[j, :, :, :last],
            send_sem=pair_send, recv_sem=pair_recv.at[j],
            device_id={"sp": me + 1 - 2 * parity}, device_id_type=MESH,
        )

    def map_copy(j, slot, last=2 * dim):
        return pltpu.make_async_remote_copy(
            src_ref=joined.at[j, :, :, :last], dst_ref=recv.at[slot, :, :, :last],
            send_sem=map_send, recv_sem=map_recv.at[slot],
            device_id={"sp": owner(2 * pair_at(j) + parity)}, device_id_type=MESH,
        )

    def by(short, work):
        pl.when(short)(lambda: work(dim))
        pl.when(jnp.logical_not(short))(lambda: work(2 * dim))

    def is_away(j):
        return owner(2 * pair_at(j) + parity) != me

    def pass_on(step):
        for index in plan[step]:
            keep, j = sequence[index]
            if not keep:
                by(me == 0, lambda last: pair_copy(index, j, last).start())

    def join(step):
        for index in plan[step]:
            keep, j = sequence[index]
            if keep:
                by(me == 1, lambda last: pair_copy(index, j, last).wait_recv())
                for h in range(per):
                    ours, theirs = spans[index, h], partner_spans[j, h]
                    early = jnp.where(parity == 1, theirs, ours)
                    late = jnp.where(parity == 1, ours, theirs)
                    both = early.astype(F32) + late.astype(F32) - dot(late[:, dim:], early)
                    joined[j, h] = both.astype(BF16)
                if j or stride > 1:
                    @pl.when(is_away(j))
                    def _():
                        by(me < 2, lambda last: map_copy(j, me // 2, last).start())

    def projection(step):
        for index in plan[step]:
            for j in range(2):
                acc = total[index, j] if index < early else None
                for d in range(1 if index < early else 0, tp):
                    for low in range(0, part, chunk):
                        piece = dot(
                            feat[d, :, low:low + chunk], weights[index, d, j, low:low + chunk, :]
                        )
                        acc = piece if acc is None else acc + piece
                        if d == tp - 1 and low + chunk == part:
                            projected[index, j] = acc.astype(BF16)
                        yield

    ticks = 2 + 3 * len(masks) + 1
    for step in range(steps):
        if step > 0:
            pass_on(step - 1)
        if 2 < step + 2 < steps:
            fetch_step(step + 2, 0, tp)
        filler, units = iter(()), 0
        if step + 1 < steps:
            skip = 1 if step == 0 else 0
            units = len(plan[step + 1]) * 2 * (tp - skip) * (part // chunk)
            if step > 0:
                fetched(step + 1, skip, tp)
            filler = projection(step + 1)
        done = [0, 0]
        when = 0
        if step == 2:
            when = 0
        elif step == steps - 1:
            when = 0
        if step > 0 and when == 0:
            join(step - 1)

        def tick():
            done[0] += 1
            if step > 0 and done[0] == when:
                join(step - 1)
            while done[1] * ticks < done[0] * units:
                done[1] += 1
                next(filler, None)

        strengths = strength_buf[...]
        rates = decay_buf[...]
        lane = lax.broadcasted_iota(jnp.int32, strengths.shape, 1)
        rest = full - 1 - me * seg - lax.broadcasted_iota(jnp.int32, (seg, 1), 0)
        rest = rest.astype(F32) * (1.0 / full)
        heads = []
        for index in plan[step]:
            keys, values = projected[index, 0], projected[index, 1]
            for h in range(per):
                head = group_at(index) * per + h
                strength = jnp.sum(jnp.where(lane == head, strengths, 0.0), axis=1, keepdims=True)
                rate = jnp.sum(jnp.where(lane[:1] == head, rates, 0.0), axis=1, keepdims=True)
                fade = jnp.exp(-rate * rest)
                cols = slice(h * dim, (h + 1) * dim)
                heads.append((keys[:, cols], values[:, cols], strength, fade))
        results = span(heads, mask_buf, eye_buf, tick)
        for _ in filler:
            pass
        for k, result in enumerate(results):
            spans[plan[step][0] + k // per, k % per] = result.astype(BF16)
    rows = dim // n

    def row_copy(q):
        return pltpu.make_async_remote_copy(
            src_ref=row_stage.at[q], dst_ref=state_out.at[0, pl.ds(mine * per, per)],
            send_sem=row_send, recv_sem=row_got,
            device_id={"sp": q}, device_id_type=MESH,
        )

    def read_copy(q):
        return pltpu.make_async_remote_copy(
            src_ref=read_stage.at[q], dst_ref=read_recv.at[mine],
            send_sem=read_send, recv_sem=read_got,
            device_id={"sp": q}, device_id_type=MESH,
        )

    unit = query_buf[0].astype(F32)
    unit = unit * lax.rsqrt(jnp.sum(unit * unit, axis=1, keepdims=True) + 1.0)
    which = lax.broadcasted_iota(jnp.int32, unit.shape, 0)
    for h in range(per):
        row = jnp.sum(jnp.where(which == mine * per + h, unit, 0.0), axis=0, keepdims=True)
        ask_buf[h] = jnp.broadcast_to(row, (dim, dim)).T
    join(steps - 1)
    recv[me // 2] = joined[0]

    def finish():
        def arrive(p):
            @pl.when(p != me // 2)
            def _():
                map_copy(0, p, 2 * dim if p else dim).wait_recv()

        arrive(0)
        states = [recv[0, h, :, :dim].astype(F32) for h in range(per)]
        for p in range(1, n // 2):
            arrive(p)
            for h in range(per):
                write, drop = recv[p, h, :, :dim].astype(F32), recv[p, h, :, dim:]
                high = states[h].astype(BF16)
                low = (states[h] - high.astype(F32)).astype(BF16)
                states[h] = states[h] + (write - dot(drop, high) - dot(drop, low))
        for h in range(per):
            cast = states[h].astype(BF16)
            for q in range(n):
                row_stage[q, h] = cast[q * rows:(q + 1) * rows]
        for d in range(n - 1, 0, -1):
            row_copy(lax.rem(me + d, n)).start()
        for h in range(per):
            raw = jnp.sum(ask_buf[h] * states[h], axis=0, keepdims=True)
            raw = raw * lax.rsqrt(jnp.mean(raw * raw, axis=1, keepdims=True) + 0.05) * gain_buf[...]
            for q in range(n):
                read_stage[q, h:h + 1] = raw
        for d in range(1, n):
            read_copy(lax.rem(me + d, n)).start()
        state_out[0, pl.ds(mine * per, per)] = row_stage[me]
        read_recv[mine] = read_stage[0]

    when_owner(finish)

    def wait_all(count):
        rows_in, reads_in = state_out.at[0, :count * per], read_recv.at[:count]
        pltpu.make_async_copy(rows_in, rows_in, row_got).wait()
        pltpu.make_async_copy(reads_in, reads_in, read_got).wait()

    def wait_sent():
        for done, sem in ((row_stage.at[1:], row_send), (read_stage.at[1:], read_send)):
            pltpu.make_async_copy(done, done, sem).wait()

    def wait_maps(low):
        if low < half:
            def wait(last):
                done = joined.at[low:, :, :, :last]
                pltpu.make_async_copy(done, done, map_send).wait()

            by(me < 2, wait)

    if stride == 1:
        wait_all(groups - 1)
    else:
        pl.when(is_owner)(lambda: wait_all(groups - 1))
        pl.when(jnp.logical_not(is_owner))(lambda: wait_all(groups))
    for g in range(groups):
        read_out[0, g * per:(g + 1) * per] = read_recv[g]
    for d in range(1, tp):
        feature_copy(d).wait_send()
    def wait_pairs(last):
        done = partner_spans.at[:, :, :, :last]
        pltpu.make_async_copy(done, done, pair_send).wait()

    by(me == 0, wait_pairs)
    if stride == 1:
        wait_maps(1)
    else:
        pl.when(is_owner)(lambda: wait_maps(1))
        pl.when(jnp.logical_not(is_owner))(lambda: wait_maps(0))
    when_owner(wait_sent)


def deliver(state, read, state_out, read_out, sem):
    copies = [
        pltpu.make_async_copy(src, dst, sem.at[k])
        for k, (src, dst) in enumerate(((state, state_out), (read, read_out)))
    ]
    for copy in copies:
        copy.start()
    for copy in copies:
        copy.wait()


def solution(mesh):
    n, tp = mesh.shape["sp"], mesh.shape["tp"]

    def shards(prompt, key_w, value_w, beta_w, bias, decay, query, gain):
        seg, part = prompt.shape[1:]
        depth = key_w.shape[0]
        heads = beta_w.shape[1]
        dim = key_w.shape[1] // heads
        per = max(1, heads // n)
        groups = heads // per
        wide = per * dim
        rows = dim // n
        block = seg // 2
        cuts = len(bounds(block))
        dma = pltpu.SemaphoreType.DMA
        vmem = pl.BlockSpec(memory_space=pltpu.VMEM)
        hbm = pl.BlockSpec(memory_space=pl.ANY)
        half = groups // 2
        found = pl.pallas_call(
            functools.partial(kernel, n, tp, groups, per, dim),
            out_shape=(
                pltpu.VMEM((1, heads, rows, dim), BF16),
                pltpu.VMEM((1, heads, dim), F32),
            ),
            in_specs=[hbm] * 8,
            out_specs=(vmem, vmem),
            scratch_shapes=[
                pltpu.VMEM((tp, seg, part), BF16),
                pltpu.VMEM((groups, tp, 2, part, wide), BF16),
                pltpu.VMEM((3, 2, seg, wide), F32),
                pltpu.VMEM((groups, 2, seg, wide), BF16),
                pltpu.VMEM((tp, heads, part), BF16),
                pltpu.VMEM((1, heads), F32),
                pltpu.VMEM((1, heads), F32),
                pltpu.VMEM((1, heads, dim), BF16),
                pltpu.VMEM((1, dim), F32),
                pltpu.VMEM((cuts, block, seg), BF16),
                pltpu.VMEM((block, seg), BF16),
                pltpu.VMEM((seg, heads), F32),
                pltpu.VMEM((groups, per, dim, 2 * dim), BF16),
                pltpu.VMEM((half, per, dim, 2 * dim), BF16),
                pltpu.VMEM((half, per, dim, 2 * dim), BF16),
                pltpu.VMEM((n // 2, per, dim, 2 * dim), BF16),
                pltpu.VMEM((per, dim, dim), F32),
                pltpu.VMEM((n, per, rows, dim), BF16),
                pltpu.VMEM((n, per, dim), F32),
                pltpu.VMEM((groups, per, dim), F32),
                dma((5,)),
                dma((tp,)),
                dma((tp - 1,)),
                dma((tp,)),
                dma((groups // 2 + 1, 2)),
                pltpu.SemaphoreType.DMA,
                dma((half,)),
                pltpu.SemaphoreType.DMA,
                dma((n // 2,)),
                pltpu.SemaphoreType.DMA,
                pltpu.SemaphoreType.DMA,
                pltpu.SemaphoreType.DMA,
                pltpu.SemaphoreType.DMA,
            ],
            compiler_params=pltpu.CompilerParams(
                collective_id=0, has_side_effects=True, vmem_limit_bytes=60 * 2**20
            ),
        )(
            prompt, key_w, value_w, beta_w.T, bias.reshape(1, heads), decay.reshape(1, heads),
            query, gain.reshape(1, dim),
        )
        return pl.pallas_call(
            deliver,
            out_shape=tuple(jax.ShapeDtypeStruct(x.shape, x.dtype) for x in found),
            in_specs=[vmem] * 2,
            out_specs=(hbm, hbm),
            scratch_shapes=[dma((2,))],
        )(*(pltpu.with_memory_space_constraint(x, pltpu.VMEM) for x in found))

    return jax.shard_map(
        shards,
        mesh=mesh,
        in_specs=(
            P("gr", "sp", "tp"),
            P(None, "tp"),
            P(None, "tp"),
            P(None, "tp"),
            P("tp"),
            P("tp"),
            P("gr", "tp", None),
            P(),
        ),
        out_specs=(P("gr", "tp", "sp", None), P("gr", "tp", None)),
        check_vma=False,
    )
```

```python
import functools

import jax
import jax.numpy as jnp
from jax import lax
from jax.experimental import pallas as pl
from jax.experimental.pallas import tpu as pltpu
from jax.sharding import PartitionSpec as P

MESH = pl.DeviceIdType.MESH
F32 = jnp.float32
BF16 = jnp.bfloat16


def dot(left, right, contract=((1,), (0,))):
    return lax.dot_general(left, right, (contract, ((), ())), preferred_element_type=F32)


def bounds(size):
    levels = (size - 1).bit_length()
    cuts = [0, min(3, levels)]
    while cuts[-1] < levels:
        cuts.append(min(cuts[-1] + 2, levels))
    return tuple(zip(cuts[:-1], cuts[1:]))


def cut_masks(size):
    row = lax.broadcasted_iota(jnp.int32, (size, 2 * size), 0)
    col = lax.rem(lax.broadcasted_iota(jnp.int32, (size, 2 * size), 1), size)
    masks = []
    for low, high in bounds(size):
        together = (row >> high) == (col >> high)
        apart = (row >> low) != (col >> low)
        masks.append((together & apart & (row > col)).astype(F32).astype(BF16))
    return masks, (row == col).astype(F32).astype(BF16)


def spread(x):
    size = x.shape[1] // 2
    zero = jnp.zeros((x.shape[0], size), x.dtype)
    return jnp.concatenate(
        [jnp.concatenate([x[:, :size], zero], axis=1), jnp.concatenate([zero, x[:, size:]], axis=1)], axis=0
    )


def under(x, y):
    return jnp.concatenate([x, y], axis=0)


def mul(x, y):
    return dot(x, spread(y)).astype(BF16)


def span(heads, masks, eye, tick):
    keys_t, rights, grams = [], [], []
    for key, value, strength, fade in heads:
        key = key.astype(F32)
        key = key * lax.rsqrt(jnp.sum(key * key, axis=1, keepdims=True) + 1.0)
        weighted = (key * strength).astype(BF16)
        value = (value.astype(F32) * (strength * fade)).astype(BF16)
        key_t = key.astype(BF16).T
        half = weighted.shape[0] // 2
        keys_t.append(key_t)
        rights.append(jnp.concatenate([value, weighted], axis=1))
        grams.append(mul(jnp.concatenate([weighted[:half], weighted[half:]], axis=1), key_t))
    cuts = masks.shape[0]
    tick()
    ns = [g * masks[0] for g in grams]
    squares = [mul(x, x) for x in ns]
    tick()
    xs = [eye[...] - x for x in ns]
    pairs = [mul(under(q, x), q) for q, x in zip(squares, xs)]
    tick()
    xs = [x + p[half:] for x, p in zip(xs, pairs)]
    xs = [x + mul(x, p[:half]) for x, p in zip(xs, pairs)]
    for cut in range(1, cuts):
        tick()
        last = cut == cuts - 1
        if last:
            both = [mul(under(g * masks[cut], k), x) for g, k, x in zip(grams, keys_t, xs)]
            ns, xs = [b[:half] for b in both], [b[half:] for b in both]
        else:
            ns = [mul(g * masks[cut], x) for g, x in zip(grams, xs)]
        tick()
        pairs = [mul(under(q, x), q) for q, x in zip(ns, xs)]
        tick()
        xs = [x - p[half:] for x, p in zip(xs, pairs)]
        xs = [x + mul(x, p[:half]) for x, p in zip(xs, pairs)]
    if cuts == 1:
        tick()
        xs = [mul(k, x) for k, x in zip(keys_t, xs)]
    tick()
    first = [dot(x[:, :half], r[:half]) for x, r in zip(xs, rights)]
    second = [dot(x[:, half:], r[half:]) for x, r in zip(xs, rights)]
    tick()
    dim = keys_t[0].shape[0]
    out = [a + b - dot(b[:, dim:].astype(BF16), a.astype(BF16)) for a, b in zip(first, second)]
    tick()
    return out


def kernel(
    n, tp, groups, per, dim,
    prompt, key_w, value_w, beta_w, bias, decay, query, gain,
    state_out, read_out,
    feat, weights, total, projected, beta_buf, bias_buf, decay_buf, query_buf, gain_buf,
    mask_buf, eye_buf, strength_buf, spans, partner_spans, joined, recv,
    ask_buf, row_stage, read_stage, read_recv,
    in_sem, beta_sem, feat_send, feat_recv, weight_sem, pair_send, pair_recv,
    map_send, map_recv, row_send, row_got, read_send, read_got,
):
    me = lax.axis_index("sp")
    core = lax.axis_index("tp")
    seg, part = prompt.shape[1], prompt.shape[2]
    wide = per * dim
    full = seg * n
    stride = n // groups
    half = groups // 2
    parity = lax.rem(me, 2)
    mine = me // stride
    chunk = min(part, 1024)

    order = list(range(half // 2, half)) + list(range(half // 2 - 1, -1, -1))
    sequence = [(0, order[0])]
    for j in range(half):
        if j + 1 < half:
            sequence.append((0, order[j + 1]))
        sequence.append((1, order[j]))
    plan = [range(1)] + [range(k, k + 2) for k in range(1, groups - 1, 2)] + [range(groups - 1, groups)]
    steps = len(plan)
    early = 1 + len(plan[1])

    def owner(g):
        return g * stride + (lax.rem(g, 2) if stride > 1 else 0)

    is_owner = me == owner(mine)

    def when_owner(work):
        if stride == 1:
            work()
        else:
            pl.when(is_owner)(work)

    def pair_at(j):
        pair = mine // 2
        if half & (half - 1):
            return lax.rem(pair + j, half)
        place = pair
        for bit in range(half.bit_length()):
            if j >> bit & 1:
                place += (1 - 2 * lax.rem(pair // 2**bit, 2)) * 2**bit
        return place

    def group_at(index):
        keep, j = sequence[index]
        return 2 * pair_at(j) + (parity if keep else 1 - parity)

    def features_of(d):
        return pl.ds(pl.multiple_of(lax.rem(core + d, tp) * part, part), part)

    def fetch_step(step, low, high):
        for d in range(low, high):
            for index in plan[step]:
                columns = pl.ds(pl.multiple_of(group_at(index) * wide, wide), wide)
                for j, w in enumerate((key_w, value_w)):
                    pltpu.make_async_copy(
                        w.at[features_of(d), columns], weights.at[index, d, j],
                        weight_sem.at[step, min(low, 1)],
                    ).start()

    def fetched(step, low, high):
        landed = weights.at[plan[step][0]:plan[step][-1] + 1, low:high]
        pltpu.make_async_copy(landed, landed, weight_sem.at[step, min(low, 1)]).wait()

    own_prompt = pltpu.make_async_copy(prompt.at[0], feat.at[0], in_sem.at[0])
    small = [
        pltpu.make_async_copy(src, dst, in_sem.at[1 + k])
        for k, (src, dst) in enumerate(
            ((bias, bias_buf), (decay, decay_buf), (query, query_buf), (gain, gain_buf))
        )
    ] + [
        pltpu.make_async_copy(beta_w.at[:, features_of(d)], beta_buf.at[d], beta_sem.at[d]) for d in range(tp)
    ]
    own_prompt.start()
    for copy in small:
        copy.start()
    fetch_step(0, 0, 1)
    fetch_step(1, 0, 1)

    partner_spans[:, :, :, dim:] = jnp.zeros((half, per, dim, dim), BF16)
    barrier = pltpu.get_barrier_semaphore()
    for d in range(1, tp):
        pl.semaphore_signal(barrier, inc=1, device_id={"tp": lax.rem(core + d, tp)}, device_id_type=MESH)
    for d in range(1, n):
        pl.semaphore_signal(barrier, inc=1, device_id={"sp": lax.rem(me + d, n)}, device_id_type=MESH)
    masks, eye = cut_masks(seg // 2)
    for k, mask in enumerate(masks):
        mask_buf[k] = mask
    eye_buf[...] = eye
    own_prompt.wait()
    pl.semaphore_wait(barrier, n - 1 + tp - 1)

    def feature_copy(d):
        return pltpu.make_async_remote_copy(
            src_ref=feat.at[0], dst_ref=feat.at[tp - d],
            send_sem=feat_send.at[d - 1], recv_sem=feat_recv.at[tp - d],
            device_id={"tp": lax.rem(core + d, tp)}, device_id_type=MESH,
        )

    for d in range(1, tp):
        feature_copy(d).start()

    def begin(step):
        fetched(step, 0, 1)
        for index in plan[step]:
            for j in range(2):
                total[index, j] = dot(feat[0], weights[index, 0, j])

    fetch_step(0, 1, tp)
    begin(0)
    fetch_step(1, 1, tp)
    begin(1)
    for copy in small:
        copy.wait()
    fetched(0, 1, tp)
    fetched(1, 1, tp)
    if steps > 2:
        fetch_step(2, 0, tp)
    for d in range(1, tp):
        feature_copy(tp - d).wait_recv()
    before = dot(feat[0], beta_buf[0], ((1,), (1,)))
    for d in range(1, tp):
        before += dot(feat[d], beta_buf[d], ((1,), (1,)))
    strength_buf[...] = jax.nn.sigmoid(before + bias_buf[...])
    for index in plan[0]:
        for j in range(2):
            acc = total[index, j]
            for d in range(1, tp):
                acc += dot(feat[d], weights[index, d, j])
            projected[index, j] = acc.astype(BF16)

    def pair_copy(index, j, last=2 * dim):
        return pltpu.make_async_remote_copy(
            src_ref=spans.at[index, :, :, :last], dst_ref=partner_spans.at[j, :, :, :last],
            send_sem=pair_send, recv_sem=pair_recv.at[j],
            device_id={"sp": me + 1 - 2 * parity}, device_id_type=MESH,
        )

    def map_copy(j, slot, last=2 * dim):
        return pltpu.make_async_remote_copy(
            src_ref=joined.at[j, :, :, :last], dst_ref=recv.at[slot, :, :, :last],
            send_sem=map_send, recv_sem=map_recv.at[slot],
            device_id={"sp": owner(2 * pair_at(j) + parity)}, device_id_type=MESH,
        )

    def by(short, work):
        pl.when(short)(lambda: work(dim))
        pl.when(jnp.logical_not(short))(lambda: work(2 * dim))

    def is_away(j):
        return owner(2 * pair_at(j) + parity) != me

    def pass_on(step):
        for index in plan[step]:
            keep, j = sequence[index]
            if not keep:
                by(me == 0, lambda last: pair_copy(index, j, last).start())

    def join(step):
        for index in plan[step]:
            keep, j = sequence[index]
            if keep:
                by(me == 1, lambda last: pair_copy(index, j, last).wait_recv())
                for h in range(per):
                    ours, theirs = spans[index, h], partner_spans[j, h]
                    early = jnp.where(parity == 1, theirs, ours)
                    late = jnp.where(parity == 1, ours, theirs)
                    both = early.astype(F32) + late.astype(F32) - dot(late[:, dim:], early)
                    joined[j, h] = both.astype(BF16)
                if j or stride > 1:
                    @pl.when(is_away(j))
                    def _():
                        by(me < 2, lambda last: map_copy(j, me // 2, last).start())

    def projection(step):
        for index in plan[step]:
            for j in range(2):
                acc = total[index, j] if index < early else None
                for d in range(1 if index < early else 0, tp):
                    for low in range(0, part, chunk):
                        piece = dot(
                            feat[d, :, low:low + chunk], weights[index, d, j, low:low + chunk, :]
                        )
                        acc = piece if acc is None else acc + piece
                        if d == tp - 1 and low + chunk == part:
                            projected[index, j] = acc.astype(BF16)
                        yield

    ticks = 2 + 3 * len(masks) + 1
    for step in range(steps):
        if step > 0:
            pass_on(step - 1)
        if 2 < step + 2 < steps:
            fetch_step(step + 2, 0, tp)
        filler, units = iter(()), 0
        if step + 1 < steps:
            skip = 1 if step == 0 else 0
            units = len(plan[step + 1]) * 2 * (tp - skip) * (part // chunk)
            if step > 0:
                fetched(step + 1, skip, tp)
            filler = projection(step + 1)
        done = [0, 0]
        when = 0
        if step == 2:
            when = 0
        elif step == steps - 1:
            when = 0
        if step > 0 and when == 0:
            join(step - 1)

        def tick():
            done[0] += 1
            if step > 0 and done[0] == when:
                join(step - 1)
            while done[1] * ticks < done[0] * units:
                done[1] += 1
                next(filler, None)

        strengths = strength_buf[...]
        rates = decay_buf[...]
        lane = lax.broadcasted_iota(jnp.int32, strengths.shape, 1)
        rest = full - 1 - me * seg - lax.broadcasted_iota(jnp.int32, (seg, 1), 0)
        rest = rest.astype(F32) * (1.0 / full)
        heads = []
        for index in plan[step]:
            keys, values = projected[index, 0], projected[index, 1]
            for h in range(per):
                head = group_at(index) * per + h
                strength = jnp.sum(jnp.where(lane == head, strengths, 0.0), axis=1, keepdims=True)
                rate = jnp.sum(jnp.where(lane[:1] == head, rates, 0.0), axis=1, keepdims=True)
                fade = jnp.exp(-rate * rest)
                cols = slice(h * dim, (h + 1) * dim)
                heads.append((keys[:, cols], values[:, cols], strength, fade))
        results = span(heads, mask_buf, eye_buf, tick)
        for _ in filler:
            pass
        for k, result in enumerate(results):
            spans[plan[step][0] + k // per, k % per] = result.astype(BF16)
    rows = dim // n

    def row_copy(q):
        return pltpu.make_async_remote_copy(
            src_ref=row_stage.at[q], dst_ref=state_out.at[0, pl.ds(mine * per, per)],
            send_sem=row_send, recv_sem=row_got,
            device_id={"sp": q}, device_id_type=MESH,
        )

    def read_copy(q):
        return pltpu.make_async_remote_copy(
            src_ref=read_stage.at[q], dst_ref=read_recv.at[mine],
            send_sem=read_send, recv_sem=read_got,
            device_id={"sp": q}, device_id_type=MESH,
        )

    unit = query_buf[0].astype(F32)
    unit = unit * lax.rsqrt(jnp.sum(unit * unit, axis=1, keepdims=True) + 1.0)
    which = lax.broadcasted_iota(jnp.int32, unit.shape, 0)
    for h in range(per):
        row = jnp.sum(jnp.where(which == mine * per + h, unit, 0.0), axis=0, keepdims=True)
        ask_buf[h] = jnp.broadcast_to(row, (dim, dim)).T
    join(steps - 1)
    recv[me // 2] = joined[0]

    def finish():
        def arrive(p):
            @pl.when(p != me // 2)
            def _():
                map_copy(0, p, 2 * dim if p else dim).wait_recv()

        arrive(0)
        states = [recv[0, h, :, :dim].astype(F32) for h in range(per)]
        for p in range(1, n // 2):
            arrive(p)
            for h in range(per):
                write, drop = recv[p, h, :, :dim].astype(F32), recv[p, h, :, dim:]
                high = states[h].astype(BF16)
                low = (states[h] - high.astype(F32)).astype(BF16)
                both = dot(jnp.concatenate([drop, drop], axis=1), under(high, low))
                states[h] = states[h] + (write - both)
        for h in range(per):
            cast = states[h].astype(BF16)
            for q in range(n):
                row_stage[q, h] = cast[q * rows:(q + 1) * rows]
        for d in range(n - 1, 0, -1):
            row_copy(lax.rem(me + d, n)).start()
        for h in range(per):
            raw = jnp.sum(ask_buf[h] * states[h], axis=0, keepdims=True)
            raw = raw * lax.rsqrt(jnp.mean(raw * raw, axis=1, keepdims=True) + 0.05) * gain_buf[...]
            for q in range(n):
                read_stage[q, h:h + 1] = raw
        for d in range(1, n):
            read_copy(lax.rem(me + d, n)).start()
        state_out[0, pl.ds(mine * per, per)] = row_stage[me]
        read_recv[mine] = read_stage[0]

    when_owner(finish)

    def wait_all(count):
        rows_in, reads_in = state_out.at[0, :count * per], read_recv.at[:count]
        pltpu.make_async_copy(rows_in, rows_in, row_got).wait()
        pltpu.make_async_copy(reads_in, reads_in, read_got).wait()

    def wait_sent():
        for done, sem in ((row_stage.at[1:], row_send), (read_stage.at[1:], read_send)):
            pltpu.make_async_copy(done, done, sem).wait()

    def wait_maps(low):
        if low < half:
            def wait(last):
                done = joined.at[low:, :, :, :last]
                pltpu.make_async_copy(done, done, map_send).wait()

            by(me < 2, wait)

    if stride == 1:
        wait_all(groups - 1)
    else:
        pl.when(is_owner)(lambda: wait_all(groups - 1))
        pl.when(jnp.logical_not(is_owner))(lambda: wait_all(groups))
    for g in range(groups):
        read_out[0, g * per:(g + 1) * per] = read_recv[g]
    for d in range(1, tp):
        feature_copy(d).wait_send()
    def wait_pairs(last):
        done = partner_spans.at[:, :, :, :last]
        pltpu.make_async_copy(done, done, pair_send).wait()

    by(me == 0, wait_pairs)
    if stride == 1:
        wait_maps(1)
    else:
        pl.when(is_owner)(lambda: wait_maps(1))
        pl.when(jnp.logical_not(is_owner))(lambda: wait_maps(0))
    when_owner(wait_sent)


def deliver(state, read, state_out, read_out, sem):
    copies = [
        pltpu.make_async_copy(src, dst, sem.at[k])
        for k, (src, dst) in enumerate(((state, state_out), (read, read_out)))
    ]
    for copy in copies:
        copy.start()
    for copy in copies:
        copy.wait()


def solution(mesh):
    n, tp = mesh.shape["sp"], mesh.shape["tp"]

    def shards(prompt, key_w, value_w, beta_w, bias, decay, query, gain):
        seg, part = prompt.shape[1:]
        depth = key_w.shape[0]
        heads = beta_w.shape[1]
        dim = key_w.shape[1] // heads
        per = max(1, heads // n)
        groups = heads // per
        wide = per * dim
        rows = dim // n
        block = seg // 2
        cuts = len(bounds(block))
        dma = pltpu.SemaphoreType.DMA
        vmem = pl.BlockSpec(memory_space=pltpu.VMEM)
        hbm = pl.BlockSpec(memory_space=pl.ANY)
        half = groups // 2
        found = pl.pallas_call(
            functools.partial(kernel, n, tp, groups, per, dim),
            out_shape=(
                pltpu.VMEM((1, heads, rows, dim), BF16),
                pltpu.VMEM((1, heads, dim), F32),
            ),
            in_specs=[hbm] * 8,
            out_specs=(vmem, vmem),
            scratch_shapes=[
                pltpu.VMEM((tp, seg, part), BF16),
                pltpu.VMEM((groups, tp, 2, part, wide), BF16),
                pltpu.VMEM((3, 2, seg, wide), F32),
                pltpu.VMEM((groups, 2, seg, wide), BF16),
                pltpu.VMEM((tp, heads, part), BF16),
                pltpu.VMEM((1, heads), F32),
                pltpu.VMEM((1, heads), F32),
                pltpu.VMEM((1, heads, dim), BF16),
                pltpu.VMEM((1, dim), F32),
                pltpu.VMEM((cuts, block, seg), BF16),
                pltpu.VMEM((block, seg), BF16),
                pltpu.VMEM((seg, heads), F32),
                pltpu.VMEM((groups, per, dim, 2 * dim), BF16),
                pltpu.VMEM((half, per, dim, 2 * dim), BF16),
                pltpu.VMEM((half, per, dim, 2 * dim), BF16),
                pltpu.VMEM((n // 2, per, dim, 2 * dim), BF16),
                pltpu.VMEM((per, dim, dim), F32),
                pltpu.VMEM((n, per, rows, dim), BF16),
                pltpu.VMEM((n, per, dim), F32),
                pltpu.VMEM((groups, per, dim), F32),
                dma((5,)),
                dma((tp,)),
                dma((tp - 1,)),
                dma((tp,)),
                dma((groups // 2 + 1, 2)),
                pltpu.SemaphoreType.DMA,
                dma((half,)),
                pltpu.SemaphoreType.DMA,
                dma((n // 2,)),
                pltpu.SemaphoreType.DMA,
                pltpu.SemaphoreType.DMA,
                pltpu.SemaphoreType.DMA,
                pltpu.SemaphoreType.DMA,
            ],
            compiler_params=pltpu.CompilerParams(
                collective_id=0, has_side_effects=True, vmem_limit_bytes=60 * 2**20
            ),
        )(
            prompt, key_w, value_w, beta_w.T, bias.reshape(1, heads), decay.reshape(1, heads),
            query, gain.reshape(1, dim),
        )
        return pl.pallas_call(
            deliver,
            out_shape=tuple(jax.ShapeDtypeStruct(x.shape, x.dtype) for x in found),
            in_specs=[vmem] * 2,
            out_specs=(hbm, hbm),
            scratch_shapes=[dma((2,))],
        )(*(pltpu.with_memory_space_constraint(x, pltpu.VMEM) for x in found))

    return jax.shard_map(
        shards,
        mesh=mesh,
        in_specs=(
            P("gr", "sp", "tp"),
            P(None, "tp"),
            P(None, "tp"),
            P(None, "tp"),
            P("tp"),
            P("tp"),
            P("gr", "tp", None),
            P(),
        ),
        out_specs=(P("gr", "tp", "sp", None), P("gr", "tp", None)),
        check_vma=False,
    )
```
